32 devices in a mesh: ep: 8 (over z, x), tp: 4 (over y, core).
Axes of the slice: x: 2, y: 2, z: 4, core: 2. Of those that a mesh axis runs over, the one named last changes fastest.
Arguments:
- tokens_a: bfloat16 [1024, 2048], P('ep'), may hold values from -6 to 6
- gain_a: float32 [2048], replicated, may hold values from 0.1 to 1.9
- value_w: bfloat16 [2048, 2048], P(None, 'tp'), may hold values from -0.125 to 0.125
- gate_w: bfloat16 [2048, 2048], P(None, 'tp'), may hold values from -0.125 to 0.125
- kernel: float32 [31, 2048], P(None, 'tp')
- chan_gain: float32 [2048], P('tp'), may hold values from 0.1 to 1.9
- out_w: bfloat16 [2048, 2048], P('tp'), may hold values from -0.125 to 0.125
- tokens_b: bfloat16 [1536, 2048], P('ep'), may hold values from -6 to 6
- gain_b: float32 [2048], replicated, may hold values from 0.1 to 1.9
- routes: int32 [1536, 2], P('ep'), may hold values from 0 to 7, all different within a row; in each aligned block of 192 rows (0 to 191, 192 to 383, ...) at most 72 rows name the same one
- route_logits: float32 [1536, 2], P('ep'), may hold values from -6 to 6
- expert_gate: bfloat16 [8, 2048, 2816], P('ep', None, 'tp'), may hold values from -0.125 to 0.125
- expert_up: bfloat16 [8, 2048, 2816], P('ep', None, 'tp'), may hold values from -0.125 to 0.125
- expert_down: bfloat16 [8, 2816, 2048], P('ep', 'tp'), may hold values from -0.109375 to 0.109375
Outputs:
- conv_out: bfloat16 [2048, 1024], P('tp', 'ep')
- moe_out: bfloat16 [2048, 1536], P('tp', 'ep')
The draws below stay inside these ranges and needn't reach their ends.
Inputs may be any that keep to these rules, and one draw needn't show every extreme that they name: `routes`: each row names 2 different experts; among the rows of one index of ep no expert is named by more than 72 rows, a bound that some block reaches.
All inputs are finite; a program needn't handle non-finite values.
Results may differ from the reference program's by a relative error of at most 0.018.
Values may be sent and summed in bfloat16 or wider, within the bound.
A program may use at most 64 MiB of HBM per device.

```python
import math
import jax
import jax.numpy as jnp
import numpy as np
from jax import lax

D = 2048
CONV_CH = 2048
KWIDTH = 31
FF = 2816
TOPK = 2
ROWS_B = 192
EXPERTS = 8
CAP = 72
TOKENS_A = 1024
TOKENS_B = 1536
N_EP = 8
N_TP = 4


def draw_kernel(key, part):
    first, second = jax.random.split(key)
    ramp = 1.0 + 3.0 * jnp.arange(CONV_CH, dtype=jnp.float32) / CONV_CH
    base = jax.random.normal(first, (KWIDTH, CONV_CH), jnp.float32)
    rough = jax.random.uniform(second, (1, CONV_CH), jnp.float32, 0.5, 1.5)
    return base * rough * ramp[None, :] / math.sqrt(KWIDTH)


def block_scale(rng, dims, pieces, smallest, high):
    def one(position, parts):
        heights = jax.random.uniform(jax.random.fold_in(jax.random.fold_in(rng, 6), position), (parts,), jnp.float32, smallest / len(pieces), high / len(pieces))
        return jnp.repeat(jnp.exp(heights), dims[position] // parts).reshape((-1,) + (1,) * (len(dims) - position - 1))

    loudness = one(*pieces[0])
    for cut in pieces[1:]:
        loudness = loudness * one(*cut)
    return loudness


def deal_out(rng, own, number, rows, amount, top, most, slope):
    order = jax.random.permutation(rng, amount)
    heavy_load, ordinary = load_shares(amount, rows * top, most, slope, True), load_shares(amount, rows * top, most, slope, False)
    places = jnp.arange(amount)

    def named(tallies, offset_by):
        used = int((tallies > 0).sum())
        fixed = max(1, used // 4)
        passed = fixed + (places - fixed + offset_by * (used - fixed)) % max(1, amount - fixed)
        return jnp.zeros((amount,), jnp.int32).at[order[jnp.where(places < fixed, places, passed)]].set(jnp.asarray(tallies, jnp.int32))

    tallies = jnp.where(number % 4 == 0, named(heavy_load, number // 4), named(ordinary, number - number // 4 - 1))
    mixed = jax.random.permutation(jax.random.fold_in(own, 3), amount)
    source_of, taker = mixed[0:amount // 2 * 2:2], mixed[1:amount // 2 * 2:2]
    room = jnp.minimum(tallies[source_of] - 1, most - tallies[taker]) // 2
    room = jnp.where((source_of == order[0]) | (taker == order[0]) | (tallies[taker] == 0), 0, jnp.maximum(room, 0))
    passed = jax.random.randint(jax.random.fold_in(own, 4), (amount // 2,), 0, 1 << 20) % (room + 1)
    tallies = tallies.at[source_of].add(-passed).at[taker].add(passed)
    members = jnp.searchsorted(jnp.cumsum(tallies), jnp.arange(rows * top), side="right").astype(jnp.int32)
    listing = members.reshape(top, rows).T
    listing = listing[jax.random.permutation(jax.random.fold_in(own, 1), rows)]
    offset_by = jax.random.randint(jax.random.fold_in(own, 2), (rows, 1), 0, top)
    return jnp.take_along_axis(listing, (jnp.arange(top)[None, :] + offset_by) % top, axis=1)


def load_shares(count, total, bound, slope, full):
    weights = [(1 << 20) // math.isqrt(grade ** slope) + 1 for grade in range(1, count + 1)]
    largest = bound if full else min(bound, max(-(-total // count), total * weights[0] // sum(weights)))
    least = 1 if total - largest >= count - 1 else 0
    counts, spare = [largest] + [least] * (count - 1), total - largest - least * (count - 1)
    while spare > 0:
        free = [i for i in range(1, count) if counts[i] < largest] or [i for i in range(1, count) if counts[i] < bound]
        pool, budget = sum([weights[i] for i in free]), spare
        for i in free:
            more = min(bound - counts[i], max(1, budget * weights[i] // pool), spare)
            counts[i] = counts[i] + more
            spare = spare - more
    return np.array(counts)


def gaussian(own_key, dims, scale, limit, cuts=(), held_as=jnp.bfloat16):
    array = scale * jax.random.normal(own_key, dims, jnp.float32)
    if cuts:
        array = array * block_scale(own_key, dims, cuts, -0.22, 0.18)
    return jnp.clip(array, -limit, limit).astype(held_as)


def setup_inputs(seed: int = 0) -> dict:
    arg_keys = jax.random.split(jax.random.key(seed), 15)
    tokens_a = gaussian(arg_keys[0], (TOKENS_A, D), 1.0, 6.0, ((0, 8),))
    gain_a = jnp.clip(1.0 + 0.18 * jax.random.normal(arg_keys[1], (D,), jnp.float32), 0.1, 1.9)
    value_w = gaussian(arg_keys[2], (D, CONV_CH), D ** -0.5, 0.125, ((1, 4),))
    gate_w = gaussian(arg_keys[3], (D, CONV_CH), D ** -0.5, 0.125, ((1, 4),))
    kernel = draw_kernel(jax.random.fold_in(arg_keys[14], 71), 0)
    chan_gain = jnp.clip(1.0 + 0.18 * jax.random.normal(arg_keys[5], (CONV_CH,), jnp.float32), 0.1, 1.9)
    out_w = gaussian(arg_keys[6], (CONV_CH, D), CONV_CH ** -0.5, 0.125, ((0, 4),))
    tokens_b = gaussian(arg_keys[7], (TOKENS_B, D), 1.0, 6.0, ((0, 8),))
    gain_b = jnp.clip(1.0 + 0.18 * jax.random.normal(arg_keys[8], (D,), jnp.float32), 0.1, 1.9)
    routes_keys = jax.random.split(jax.random.fold_in(arg_keys[9], 1), TOKENS_B // ROWS_B)
    routes_turns = jax.random.permutation(jax.random.fold_in(arg_keys[9], 3), TOKENS_B // ROWS_B)
    routes = jax.vmap(lambda own, number: deal_out(jax.random.fold_in(arg_keys[9], 2), own, number, ROWS_B, EXPERTS, TOPK, CAP, 1))(routes_keys, routes_turns).reshape((TOKENS_B, TOPK))
    route_logits = gaussian(arg_keys[10], (TOKENS_B, TOPK), 1.0, 6.0, ((0, 8),), jnp.float32)
    expert_gate = gaussian(arg_keys[11], (EXPERTS, D, FF), D ** -0.5, 0.125, ((0, 8), (2, 4)))
    expert_up = gaussian(arg_keys[12], (EXPERTS, D, FF), D ** -0.5, 0.125, ((0, 8), (2, 4)))
    expert_down = gaussian(arg_keys[13], (EXPERTS, FF, D), FF ** -0.5, 0.109375, ((0, 8), (1, 4)))
    return dict(tokens_a=tokens_a, gain_a=gain_a, value_w=value_w, gate_w=gate_w, kernel=kernel, chan_gain=chan_gain, out_w=out_w, tokens_b=tokens_b, gain_b=gain_b, routes=routes, route_logits=route_logits, expert_gate=expert_gate, expert_up=expert_up, expert_down=expert_down)


def rms_scaled(tokens, gain):
    values = tokens.astype(jnp.float32)
    scaled = values * lax.rsqrt(lax.optimization_barrier(jnp.mean(values * values, axis=1, keepdims=True)) + 1e-06)
    return (scaled * gain[None, :]).astype(jnp.bfloat16)

def slot_table(route_rows, experts, capacity):
    flat_expert = route_rows.reshape(-1).astype(jnp.int32)
    expert_ids = jnp.arange(experts, dtype=jnp.int32)
    onehot = (flat_expert[:, None] == expert_ids[None, :]).astype(jnp.int32)
    before = jnp.cumsum(onehot, axis=0).astype(jnp.int32) - onehot
    ranking = lax.optimization_barrier(jnp.sum(before * onehot, axis=1)).astype(jnp.int32)
    return (flat_expert * capacity + ranking).astype(jnp.int32)

def reference(tokens_a, gain_a, value_w, gate_w, kernel, chan_gain, out_w, tokens_b, gain_b, routes, route_logits, expert_gate, expert_up, expert_down):
    normed = rms_scaled(tokens_a, gain_a)
    value_part = jnp.dot(normed, value_w, preferred_element_type=jnp.float32)
    gate_part = jnp.dot(normed, gate_w, preferred_element_type=jnp.float32)
    glu = (value_part * jax.nn.sigmoid(gate_part)).astype(jnp.bfloat16)
    glu = lax.optimization_barrier(glu).astype(jnp.float32)
    length = glu.shape[0]
    padded = jnp.concatenate([jnp.zeros((KWIDTH - 1, CONV_CH), jnp.float32), glu], axis=0)
    mixed = jnp.zeros((length, CONV_CH), jnp.float32)
    for tap in range(KWIDTH):
        mixed = mixed + kernel[tap][None, :] * padded[tap:tap + length]
    average = lax.optimization_barrier(jnp.mean(mixed, axis=1, keepdims=True))
    spread = lax.optimization_barrier(jnp.mean(mixed * mixed, axis=1, keepdims=True)) - average * average
    activated = jax.nn.silu((mixed - average) * lax.rsqrt(spread + 1e-05) * chan_gain[None, :]).astype(jnp.bfloat16)
    group = CONV_CH // N_TP
    conv_sum = jnp.zeros((length, D), jnp.float32)
    for index in range(N_TP):
        partial_term = jnp.dot(activated[:, index * group:(index + 1) * group], out_w[index * group:(index + 1) * group], preferred_element_type=jnp.float32).astype(jnp.bfloat16)
        conv_sum = conv_sum + lax.optimization_barrier(partial_term).astype(jnp.float32)
    conv_out = conv_sum.astype(jnp.bfloat16).T
    normed_b = rms_scaled(tokens_b, gain_b)
    per_block = TOKENS_B // N_EP
    route_blocks = routes.reshape(N_EP, per_block, TOPK)

    def block_slots(route_rows):
        return slot_table(route_rows, EXPERTS, CAP)
    slot_blocks = jax.vmap(block_slots)(route_blocks)
    block_ids = jnp.arange(N_EP, dtype=jnp.int32)
    owners = (jnp.arange(per_block * TOPK, dtype=jnp.int32) // TOPK)[None, :] + block_ids[:, None] * per_block

    def block_fill(slots, owner_rows):
        return jnp.zeros((EXPERTS * CAP,), jnp.int32).at[slots].set(owner_rows + 1)
    filled = jax.vmap(block_fill)(slot_blocks, owners)
    index_table = jnp.transpose(filled.reshape(N_EP, EXPERTS, CAP), (1, 0, 2)).reshape(EXPERTS, N_EP * CAP) - 1
    group_ff = FF // N_TP

    def expert_apply(operands):
        index_rows, gate_e, up_e, down_e = operands
        picked = jnp.take(normed_b, jnp.maximum(index_rows, 0), axis=0)
        picked = jnp.where((index_rows >= 0)[:, None], picked, jnp.zeros_like(picked))
        gate_act = jnp.dot(picked, gate_e, preferred_element_type=jnp.float32)
        up_act = jnp.dot(picked, up_e, preferred_element_type=jnp.float32)
        hidden = (jax.nn.silu(gate_act) * up_act).astype(jnp.bfloat16)
        hidden_groups = hidden.reshape(-1, N_TP, group_ff).astype(jnp.float32)
        down_groups = down_e.reshape(N_TP, group_ff, D).astype(jnp.float32)
        partial_terms = jnp.einsum('sgf,gfd->gsd', hidden_groups, down_groups).astype(jnp.bfloat16)
        partial_terms = lax.optimization_barrier(partial_terms)
        return lax.optimization_barrier(jnp.sum(partial_terms.astype(jnp.float32), axis=0)).astype(jnp.bfloat16)
    results = lax.map(expert_apply, (index_table, expert_gate, expert_up, expert_down))
    results_flat = results.reshape(EXPERTS * N_EP * CAP, D)
    expert_flat = route_blocks.reshape(N_EP, per_block * TOPK)
    ranking = slot_blocks - expert_flat * CAP
    flat_index = expert_flat * (N_EP * CAP) + block_ids[:, None] * CAP + ranking
    values = jnp.take(results_flat, flat_index.reshape(-1), axis=0).astype(jnp.float32).reshape(TOKENS_B, TOPK, D)
    weights = jax.nn.softmax(route_logits, axis=1)
    moe_out = lax.optimization_barrier(jnp.sum(weights[:, :, None] * values, axis=1)).astype(jnp.bfloat16).T
    return (conv_out, moe_out)
```

```python
import functools

import jax
import jax.numpy as jnp
from jax import lax
from jax.experimental import pallas as pl
from jax.experimental.pallas import tpu as pltpu
from jax.sharding import PartitionSpec as P

MESH = pl.DeviceIdType.MESH
F32 = jnp.float32
BF16 = jnp.bfloat16
HALO = 32


def mm(a, b):
    return jnp.dot(a, b, preferred_element_type=F32)


def mt(a, b):
    return lax.dot_general(a, b, (((1,), (1,)), ((), ())), preferred_element_type=F32)


def kernel_body(
    n, ny, cap, groups, channels,
    tokens_a_h, gain_a, value_h, gate_h, taps, chan_gain, out_h,
    tokens_b_h, gain_b, routes, logits, eg_h, eu_h, ed_h,
    conv_o, moe_o,
    tok_a, tok_b, val_w, gat_w, out_w, eg, eu, ed,
    send, xbuf, gacc, uacc, hid, down_s, down_r, down_m, pair, yrecv, ret_s, ret_r,
    pad, tail, halo, st_s, st_r, st_ys, st_yr, conv_s, conv_r, conv_m, conv_p, conv_y,
    loc, a2a_ss, a2a_rs, fw_ss, fw_rs, ya_ss, ya_rs, yf_ss, yf_rs,
    dp_ss, dp_rs, dy_ss, dy_rs, rt_ss, rt_rs, one_ss, one_rs,
    sy_ss, sy_rs, cp_ss, cp_rs, cy_ss, cy_rs,
):
    e = lax.axis_index("ep")
    t = lax.axis_index("tp")
    y = t // 2
    c = t % 2
    partner = (e, y * 2 + (1 - c))
    feats = xbuf.shape[3]
    rows = n * cap
    per = n // groups

    def ep_peer(d):
        return (lax.rem(e + d, n), t)

    def y_peer(m):
        return (e, lax.rem(y + m, ny) * 2 + c)

    def remote(src, dst, ss, rs, device):
        return pltpu.make_async_remote_copy(
            src_ref=src, dst_ref=dst, send_sem=ss, recv_sem=rs, device_id=device, device_id_type=MESH
        )

    pairs = [(tokens_b_h, tok_b), (tokens_a_h, tok_a), (value_h, val_w), (gate_h, gat_w),
             (eg_h.at[0], eg), (eu_h.at[0], eu), (out_h, out_w), (ed_h.at[0], ed)]
    local = [pltpu.make_async_copy(src, dst, loc.at[i]) for i, (src, dst) in enumerate(pairs)]
    for copy in local:
        copy.start()

    barrier = pltpu.get_barrier_semaphore()
    for d in range(1, n):
        pl.semaphore_signal(barrier, inc=1, device_id=ep_peer(d), device_id_type=MESH)
    pl.semaphore_signal(barrier, inc=1, device_id=partner, device_id_type=MESH)
    for m in range(1, ny):
        pl.semaphore_signal(barrier, inc=1, device_id=y_peer(m), device_id_type=MESH)

    count = tok_b.shape[0]
    rel = routes[...] - e
    rel = jnp.where(rel < 0, rel + n, rel).astype(F32)
    row = lax.broadcasted_iota(jnp.int32, (count, count), 0)
    col = lax.broadcasted_iota(jnp.int32, (count, count), 1)

    def upright(line):
        return jnp.sum(jnp.where(row == col, line, 0.0), axis=1, keepdims=True)

    rel0, rel1 = upright(rel[0:1]), upright(rel[1:2])
    expert = lax.broadcasted_iota(jnp.int32, (count, n), 1).astype(F32)
    is0, is1 = expert == rel0, expert == rel1
    named = (jnp.where(is0, 1.0, 0.0) + jnp.where(is1, 1.0, 0.0)).astype(BF16)
    before = mm(jnp.where(row > col, 1.0, 0.0).astype(BF16), named)
    slot0 = rel0 * cap + jnp.sum(jnp.where(is0, before, 0.0), axis=1, keepdims=True)
    slot1 = rel1 * cap + jnp.sum(jnp.where(is1, before, 0.0), axis=1, keepdims=True)
    across0 = jnp.sum(jnp.where(row == col, slot0, 0.0), axis=0, keepdims=True)
    across1 = jnp.sum(jnp.where(row == col, slot1, 0.0), axis=0, keepdims=True)
    ids = lax.broadcasted_iota(jnp.int32, (rows, count), 0).astype(F32)
    pick = jnp.where((ids == across0) | (ids == across1), 1.0, 0.0).astype(BF16)

    local[0].wait()
    whole = tok_b[...].astype(F32)
    scale = lax.rsqrt(jnp.mean(whole * whole, axis=1, keepdims=True) + 1e-06)
    own_cols = pl.ds(pl.multiple_of(t * feats, feats), feats)
    mine = (tok_b[:, own_cols].astype(F32) * scale * gain_b[:, own_cols]).astype(BF16)
    picked = mm(pick, mine).reshape(n, cap, feats).astype(BF16)
    send[...] = picked
    xbuf[t, 0] = picked[0]

    pl.semaphore_wait(barrier, n + ny - 1)
    a2a = {}
    for d in range(1, n):
        a2a[d] = remote(send.at[d], xbuf.at[t, d], a2a_ss.at[d], a2a_rs.at[d], ep_peer(d))
        a2a[d].start()

    forwards, crossings, onward = [], {}, []

    def arrive(upto):
        for g in range(len(forwards), min(upto, groups)):
            for d in range(max(1, g * per), (g + 1) * per):
                a2a[d].wait_recv()
            part = xbuf.at[t, pl.ds(g * per, per)]
            for m in range(1, ny):
                copy = remote(part, part, ya_ss.at[m, g], ya_rs.at[m, g], y_peer(m))
                copy.start()
                crossings[m, g] = copy
            copy = remote(part, part, fw_ss.at[g], fw_rs.at[g], partner)
            copy.start()
            forwards.append(copy)

    def hand_on(upto):
        for g in range(len(onward), min(upto, groups)):
            copies = []
            for m in range(1, ny):
                crossings[m, g].wait_recv()
                block = lax.rem(y + ny - m, ny) * 2 + c
                part = xbuf.at[block, pl.ds(g * per, per)]
                copy = remote(part, part, yf_ss.at[m, g], yf_rs.at[m, g], partner)
                copy.start()
                copies.append(copy)
            onward.append(copies)

    cut = max(1, groups // 2)
    spans = [(0, cut), (cut, groups)]

    def project(block, h, first=False):
        lo, hi = spans[h][0] * per, spans[h][1] * per
        x = xbuf[block, pl.ds(lo, hi - lo)].astype(F32).reshape((hi - lo) * cap, feats).astype(BF16)
        at = pl.ds(pl.multiple_of(block * feats, feats), feats)
        to = pl.ds(lo * cap, (hi - lo) * cap)
        if first:
            gacc[to, :] = mt(x, eg[:, at])
            uacc[to, :] = mt(x, eu[:, at])
        else:
            gacc[to, :] += mt(x, eg[:, at])
            uacc[to, :] += mt(x, eu[:, at])

    def out_cols(m, core):
        block = lax.rem(y + m, ny) * 2 + core
        return pl.ds(pl.multiple_of(block * feats, feats), feats)

    down_x, down_y, returns = {}, {}, []
    order = list(range(1, ny)) + [0]

    def down(h):
        lo, hi = spans[h][0] * per, spans[h][1] * per
        to = pl.ds(lo * cap, (hi - lo) * cap)
        at = pl.ds(lo, hi - lo)
        hid[to, :] = (jax.nn.silu(gacc[to, :]) * uacc[to, :]).astype(BF16)
        for m in order:
            down_s[m, at] = mm(hid[to, :], ed[:, out_cols(m, 1 - c)]).reshape(hi - lo, cap, feats).astype(BF16)
            copy = remote(down_s.at[m, at], down_r.at[m, at], dp_ss.at[m, h], dp_rs.at[m, h], partner)
            copy.start()
            down_x[m, h] = copy
            down_m[m, at] = mm(hid[to, :], ed[:, out_cols(m, c)]).reshape(hi - lo, cap, feats)

    def cross(h):
        for m in order[:-1]:
            down_x[m, h].wait_recv()
        for g in range(*spans[h]):
            at = pl.ds(g * per, per)
            for m in order[:-1]:
                pair[m, at] = (down_m[m, at] + down_r[m, at].astype(F32)).astype(BF16)
                copy = remote(pair.at[m, at], yrecv.at[m, at], dy_ss.at[m, g], dy_rs.at[m, g], y_peer(m))
                copy.start()
                down_y[m, g] = copy
        down_x[0, h].wait_recv()

    def give_back(first, last):
        for g in range(first, last):
            at = pl.ds(g * per, per)
            summed = down_m[0, at] + down_r[0, at].astype(F32)
            for m in range(1, ny):
                down_y[m, g].wait_recv()
                summed = summed + yrecv[m, at].astype(F32)
            ret_s[at] = summed.astype(BF16)
            for d in range(g * per, (g + 1) * per):
                if d == 0:
                    ret_r[0] = summed[0].astype(BF16)
                else:
                    copy = remote(ret_s.at[d], ret_r.at[d], rt_ss.at[d], rt_rs.at[d], ep_peer(n - d))
                    copy.start()
                    returns.append(copy)

    def block_of(m, core):
        return lax.rem(y + ny - m, ny) * 2 + core

    arrive(1)

    local[1].wait()
    whole = tok_a[...].astype(F32)
    scale = lax.rsqrt(jnp.mean(whole * whole, axis=1, keepdims=True) + 1e-06)
    normed = (whole * scale * gain_a[...]).astype(BF16)
    local[2].wait()
    value = mm(normed, val_w[...])
    local[3].wait()
    glu = (value * jax.nn.sigmoid(mm(normed, gat_w[...]))).astype(BF16)
    length = glu.shape[0]
    tail[...] = glu[length - HALO:]
    rim = remote(tail, halo, one_ss.at[0], one_rs.at[0], ep_peer(1))
    rim.start()
    pad[HALO:] = glu.astype(F32)

    arrive(3)
    hand_on(1)
    arrive(4)
    hand_on(2)

    rim.wait_recv()
    pad[:HALO] = jnp.where(e > 0, halo[...].astype(F32), 0.0)
    width = taps.shape[0]
    chunk = min(128, pad.shape[1])
    total = jnp.zeros((length, 1), F32)
    square = jnp.zeros((length, 1), F32)
    mixed = []
    for lane in range(0, pad.shape[1], chunk):
        acc = jnp.zeros((length, chunk), F32)
        for tap in range(width):
            at = HALO - width + 1 + tap
            acc = acc + taps[tap:tap + 1, lane:lane + chunk] * pad[at:at + length, lane:lane + chunk]
        total = total + jnp.sum(acc, axis=1, keepdims=True)
        square = square + jnp.sum(acc * acc, axis=1, keepdims=True)
        mixed.append(acc)
    mixed = jnp.concatenate(mixed, axis=1)
    lanes = lax.broadcasted_iota(jnp.int32, (length, 128), 1)
    stats = jnp.where(lanes < 4, total, square).T
    st_s[...] = stats[0:8]
    stat = remote(st_s, st_r, one_ss.at[1], one_rs.at[1], partner)
    stat.start()

    arrive(5)
    hand_on(3)
    local[4].wait()
    local[5].wait()
    project(t, 0, True)
    arrive(6)
    hand_on(4)
    arrive(max(cut, min(6, groups)))
    hand_on(cut)

    stat.wait_recv()
    st_ys[...] = st_s[...] + st_r[...]
    stat_y = []
    for m in range(1, ny):
        copy = remote(st_ys, st_yr.at[m], sy_ss.at[m], sy_rs.at[m], y_peer(m))
        copy.start()
        stat_y.append(copy)

    for m in range(1, ny):
        project(block_of(m, c), 0)
    for g in range(cut):
        forwards[g].wait_recv()
    project(block_of(0, 1 - c), 0)
    arrive(7)
    hand_on(5)
    for g in range(cut):
        for copy in onward[g]:
            copy.wait_recv()
    for m in range(1, ny):
        project(block_of(m, 1 - c), 0)
    arrive(groups)
    hand_on(6)
    local[7].wait()
    down(0)
    hand_on(7)
    cross(0)

    sums = st_ys[...]
    for m in range(1, ny):
        stat_y[m - 1].wait_recv()
        sums = sums + st_yr[m]
    back = jnp.concatenate([sums] * (length // 8), axis=0).T
    average = back[:, 0:1] / channels
    spread = back[:, 4:5] / channels - average * average
    act = jax.nn.silu((mixed - average) * lax.rsqrt(spread + 1e-05) * chan_gain[...]).astype(BF16)
    local[6].wait()
    hand_on(groups)

    conv_x = []
    for m in range(ny):
        conv_s[m] = mm(act, out_w[:, out_cols(m, 1 - c)]).astype(BF16)
        copy = remote(conv_s.at[m], conv_r.at[m], cp_ss.at[m], cp_rs.at[m], partner)
        copy.start()
        conv_x.append(copy)
        conv_m[m] = mm(act, out_w[:, out_cols(m, c)])

    project(t, 1, True)
    for m in range(1, ny):
        project(block_of(m, c), 1)
    for g in range(cut, groups):
        forwards[g].wait_recv()
    project(block_of(0, 1 - c), 1)
    for g in range(cut, groups):
        for copy in onward[g]:
            copy.wait_recv()
    for m in range(1, ny):
        project(block_of(m, 1 - c), 1)
    give_back(0, cut // 2)
    down(1)
    cross(1)
    give_back(cut // 2, cut)

    conv_cross = []
    for m in range(ny):
        conv_x[m].wait_recv()
        summed = conv_m[m] + conv_r[m].astype(F32)
        if m == 0:
            conv_m[0] = summed
        else:
            conv_p[m] = summed.astype(BF16)
            copy = remote(conv_p.at[m], conv_y.at[m], cy_ss.at[m], cy_rs.at[m], y_peer(m))
            copy.start()
            conv_cross.append(copy)
    give_back(cut, groups)

    result = conv_m[0]
    for m in range(1, ny):
        conv_cross[m - 1].wait_recv()
        result = result + conv_y[m].astype(F32)
    conv_o[...] = result.astype(BF16)

    logit = logits[...]
    top = jnp.max(logit, axis=0, keepdims=True)
    exps = jnp.exp(logit - top)
    weight = exps / jnp.sum(exps, axis=0, keepdims=True)
    weight0, weight1 = upright(weight[0:1]), upright(weight[1:2])
    slots = lax.broadcasted_iota(jnp.int32, (count, rows), 1).astype(F32)
    combine = jnp.where(slots == slot0, weight0, 0.0) + jnp.where(slots == slot1, weight1, 0.0)
    high = combine.astype(BF16)
    low = (combine - high.astype(F32)).astype(BF16)
    for copy in returns:
        copy.wait_recv()
    returned = ret_r[...].astype(F32).reshape(rows, feats).astype(BF16)
    moe_o[...] = (mm(high, returned) + mm(low, returned)).astype(BF16)

    sent = list(a2a.values()) + forwards + list(crossings.values()) + [rim, stat] + stat_y + conv_x
    sent += sum(onward, []) + conv_cross + list(down_x.values()) + list(down_y.values()) + returns
    for copy in sent:
        copy.wait_send()


def solution(mesh):
    n = mesh.shape["ep"]
    n_tp = mesh.shape["tp"]
    ny = n_tp // 2
    groups = min(n, 8)

    def body(tokens_a, gain_a, value_w, gate_w, kernel, chan_gain, out_w,
             tokens_b, gain_b, routes, logits, eg, eu, ed):
        len_a, model = tokens_a.shape
        len_b = tokens_b.shape[0]
        chans = value_w.shape[1]
        feats = model // n_tp
        hidden = eg.shape[2]
        cap = 3 * len_b * routes.shape[1] // (2 * n)
        cap = -(-cap // 8) * 8
        rows = n * cap
        dma = pltpu.SemaphoreType.DMA
        vmem = pltpu.VMEM
        blocks = (n, cap, feats)
        scratch = [
            vmem((len_a, model), BF16), vmem((len_b, model), BF16),
            vmem((model, chans), BF16), vmem((model, chans), BF16), vmem((chans, model), BF16),
            vmem((hidden, model), BF16), vmem((hidden, model), BF16), vmem((hidden, model), BF16),
            vmem(blocks, BF16), vmem((n_tp,) + blocks, BF16),
            vmem((rows, hidden), F32), vmem((rows, hidden), F32), vmem((rows, hidden), BF16),
            vmem((ny,) + blocks, BF16), vmem((ny,) + blocks, BF16), vmem((ny,) + blocks, F32),
            vmem((ny,) + blocks, BF16), vmem((ny,) + blocks, BF16),
            vmem(blocks, BF16), vmem(blocks, BF16),
            vmem((HALO + len_a, chans), F32), vmem((HALO, chans), BF16), vmem((HALO, chans), BF16),
            vmem((8, len_a), F32), vmem((8, len_a), F32), vmem((8, len_a), F32), vmem((ny, 8, len_a), F32),
            vmem((ny, len_a, feats), BF16), vmem((ny, len_a, feats), BF16), vmem((ny, len_a, feats), F32),
            vmem((ny, len_a, feats), BF16), vmem((ny, len_a, feats), BF16),
            dma((8,)), dma((n,)), dma((n,)), dma((groups,)), dma((groups,)),
            dma((ny, groups)), dma((ny, groups)), dma((ny, groups)), dma((ny, groups)),
            dma((ny, 2)), dma((ny, 2)), dma((ny, groups)), dma((ny, groups)), dma((n,)), dma((n,)),
            dma((2,)), dma((2,)),
            dma((ny,)), dma((ny,)), dma((ny,)), dma((ny,)), dma((ny,)), dma((ny,)),
        ]
        hbm = pl.BlockSpec(memory_space=pl.ANY)
        near = pl.BlockSpec(memory_space=vmem)
        conv, moe = pl.pallas_call(
            functools.partial(kernel_body, n, ny, cap, groups, chans * n_tp),
            out_shape=(
                vmem((len_a, feats), BF16),
                vmem((len_b, feats), BF16),
            ),
            in_specs=[hbm, near, hbm, hbm, near, near, hbm, hbm, near, near, near, hbm, hbm, hbm],
            out_specs=(near, near),
            scratch_shapes=scratch,
            compiler_params=pltpu.CompilerParams(
                collective_id=0, has_side_effects=True, vmem_limit_bytes=62914560
            ),
        )(tokens_a, gain_a[None, :], value_w, gate_w, kernel, chan_gain[None, :], out_w,
          tokens_b, gain_b[None, :], routes.T, logits.T, eg.swapaxes(1, 2), eu.swapaxes(1, 2), ed)

        def finish(conv_i, moe_i, conv_f, moe_f):
            conv_f[...] = conv_i[...].T
            moe_f[...] = moe_i[...]

        conv, moe = pl.pallas_call(
            finish,
            out_shape=(
                jax.ShapeDtypeStruct((feats, len_a), BF16),
                jax.ShapeDtypeStruct((len_b, feats), BF16),
            ),
            in_specs=[near, near],
            out_specs=(near, near),
            compiler_params=pltpu.CompilerParams(vmem_limit_bytes=4 * 1024 * 1024),
        )(conv, moe)
        return conv, moe.T

    return jax.shard_map(
        body,
        mesh=mesh,
        in_specs=(
            P("ep", None), P(), P(None, "tp"), P(None, "tp"), P(None, "tp"), P("tp"), P("tp", None),
            P("ep", None), P(), P("ep", None), P("ep", None),
            P("ep", None, "tp"), P("ep", None, "tp"), P("ep", "tp", None),
        ),
        out_specs=(P("tp", "ep"), P("tp", "ep")),
        check_vma=False,
    )
```

```python
import functools

import jax
import jax.numpy as jnp
from jax import lax
from jax.experimental import pallas as pl
from jax.experimental.pallas import tpu as pltpu
from jax.sharding import PartitionSpec as P

MESH = pl.DeviceIdType.MESH
F32 = jnp.float32
BF16 = jnp.bfloat16
HALO = 32


def mm(a, b):
    return jnp.dot(a, b, preferred_element_type=F32)


def mt(a, b):
    return lax.dot_general(a, b, (((1,), (1,)), ((), ())), preferred_element_type=F32)


def kernel_body(
    n, ny, cap, groups, near_groups, chunks, channels,
    tokens_a_h, gain_a_h, value_h, gate_h, taps_h, chan_gain_h, out_h,
    tokens_b_h, gain_b_h, routes_h, logits_h, eg_h, eu_h, ed_h,
    conv_o, moe_o,
    tok_a, tok_b, val_w, gat_w, out_w, eg, eu, ed, gain_a, gain_b, taps, chan_gain, routes, logits,
    send, nsend, xbuf, gacc, uacc, down_s, down_r, down_m, pair, yrecv, ret_s, ret_r,
    pad, tail, halo, st_s, st_r, st_ys, st_yr, conv_s, conv_r, conv_m, conv_p, conv_y,
    loc, a2a_ss, a2a_rs, nr_ss, nr_rs, fw_ss, fw_rs, ya_ss, ya_rs,
    dp_ss, dp_rs, dy_ss, dy_rs, rt_ss, rt_rs, one_ss, one_rs,
    sy_ss, sy_rs, cp_ss, cp_rs, cy_ss, cy_rs,
):
    e = lax.axis_index("ep")
    t = lax.axis_index("tp")
    y = t // 2
    c = t % 2
    partner = (e, y * 2 + (1 - c))
    feats = xbuf.shape[3]
    rows = n * cap
    per = n // groups
    near = near_groups * per

    def flip(v, d):
        bit = 1
        while bit <= d:
            if d & bit:
                v = v + bit - 2 * bit * lax.rem(v // bit, 2)
            bit *= 2
        return v

    def ep_peer(d):
        return (flip(e, d), t)

    def y_peer(m):
        return (e, lax.rem(y + m, ny) * 2 + c)

    def block_of(m, core):
        return lax.rem(y + ny - m, ny) * 2 + core

    def cols_of(block):
        return pl.ds(pl.multiple_of(block * feats, feats), feats)

    def remote(src, dst, ss, rs, device):
        return pltpu.make_async_remote_copy(
            src_ref=src, dst_ref=dst, send_sem=ss, recv_sem=rs, device_id=device, device_id_type=MESH
        )

    pairs = dict(
        routes=(routes_h, routes), tok_b=(tokens_b_h, tok_b), gain_b=(gain_b_h, gain_b),
        tok_a=(tokens_a_h, tok_a), gain_a=(gain_a_h, gain_a), val=(value_h, val_w), gat=(gate_h, gat_w),
        eg=(eg_h.at[0], eg), eu=(eu_h.at[0], eu), ed=(ed_h.at[0], ed), taps=(taps_h, taps),
        chan=(chan_gain_h, chan_gain), out=(out_h, out_w), logits=(logits_h, logits),
    )
    local = {
        name: pltpu.make_async_copy(src, dst, loc.at[i]) for i, (name, (src, dst)) in enumerate(pairs.items())
    }
    for name in ("routes", "tok_b", "gain_b"):
        local[name].start()

    barrier = pltpu.get_barrier_semaphore()
    for d in range(n - 1, 0, -1):
        pl.semaphore_signal(barrier, inc=1, device_id=ep_peer(d), device_id_type=MESH)
    pl.semaphore_signal(barrier, inc=1, device_id=partner, device_id_type=MESH)
    for m in range(1, ny):
        pl.semaphore_signal(barrier, inc=1, device_id=y_peer(m), device_id_type=MESH)
    for name in list(pairs)[3:]:
        local[name].start()

    count = tok_b.shape[0]
    row = lax.broadcasted_iota(jnp.int32, (count, count), 0)
    col = lax.broadcasted_iota(jnp.int32, (count, count), 1)

    def upright(line):
        return jnp.sum(jnp.where(row == col, line, 0.0), axis=1, keepdims=True)

    local["routes"].wait()
    rel = jnp.bitwise_xor(routes[...], e).astype(F32)
    rel0, rel1 = upright(rel[0:1]), upright(rel[1:2])
    expert = lax.broadcasted_iota(jnp.int32, (count, n), 1).astype(F32)
    is0, is1 = expert == rel0, expert == rel1
    named = (jnp.where(is0, 1.0, 0.0) + jnp.where(is1, 1.0, 0.0)).astype(BF16)
    before = mm(jnp.where(row > col, 1.0, 0.0).astype(BF16), named)
    slot0 = rel0 * cap + jnp.sum(jnp.where(is0, before, 0.0), axis=1, keepdims=True)
    slot1 = rel1 * cap + jnp.sum(jnp.where(is1, before, 0.0), axis=1, keepdims=True)
    across0 = jnp.sum(jnp.where(row == col, slot0, 0.0), axis=0, keepdims=True)
    across1 = jnp.sum(jnp.where(row == col, slot1, 0.0), axis=0, keepdims=True)

    def picker(lines):
        ids = lax.broadcasted_iota(jnp.int32, (lines, count), 0).astype(F32)
        return jnp.where((ids == across0) | (ids == across1), 1.0, 0.0).astype(BF16)

    pick = picker(rows)

    local["tok_b"].wait()
    local["gain_b"].wait()
    whole = tok_b[...].astype(F32)
    scale_b = lax.rsqrt(jnp.mean(whole * whole, axis=1, keepdims=True) + 1e-06)

    def normed_b(block):
        at = cols_of(block)
        return (tok_b[:, at].astype(F32) * scale_b * gain_b[:, at]).astype(BF16)

    picked = mm(pick, normed_b(t)).reshape(n, cap, feats).astype(BF16)
    send[...] = picked
    xbuf[t, 0] = picked[0]

    pl.semaphore_wait(barrier, n + ny - 1)
    a2a, nears, crossings, forwards = {}, {}, {}, {}
    k0, k1, k2, k3 = chunks

    def dispatch(k):
        for d in range(max(1, k[0] * per), k[1] * per):
            a2a[d] = remote(send.at[d], xbuf.at[t, d], a2a_ss.at[d], a2a_rs.at[d], ep_peer(d))
            a2a[d].start()

    dispatch((0, near_groups))
    dispatch(k2)
    dispatch((near_groups, k1[1]))

    pick_near, pick_own = picker(near * cap), picker(cap)
    for m in range(1, ny):
        block = block_of(m, c)
        picked = mm(pick_near, normed_b(block)).reshape(near, cap, feats).astype(BF16)
        nsend[m] = picked
        xbuf[block, 0] = picked[0]
        for d in range(1, near):
            copy = remote(nsend.at[m, d], xbuf.at[block, d], nr_ss.at[m, d], nr_rs.at[m, d], ep_peer(d))
            copy.start()
            nears[m, d] = copy
    for m in range(ny):
        block = block_of(m, 1 - c)
        xbuf[block, 0] = mm(pick_own, normed_b(block)).astype(BF16)

    def span(g):
        return max(1, g * per), (g + 1) * per

    def forward(m, g):
        lo, hi = span(g)
        if lo < hi:
            part = xbuf.at[block_of(m, c), pl.ds(lo, hi - lo)]
            copy = remote(part, part, fw_ss.at[m, g], fw_rs.at[m, g], partner)
            copy.start()
            forwards[m, g] = copy

    def arrive(g):
        lo, hi = span(g)
        for d in range(lo, hi):
            a2a[d].wait_recv()
        if g >= near_groups:
            part = xbuf.at[t, pl.ds(lo, hi - lo)]
            for m in range(1, ny):
                copy = remote(part, part, ya_ss.at[m, g], ya_rs.at[m, g], y_peer(m))
                copy.start()
                crossings[m, g] = copy
        forward(0, g)

    def hand_on(g):
        for m in range(1, ny):
            if g >= near_groups:
                crossings[m, g].wait_recv()
            else:
                for d in range(*span(g)):
                    nears[m, d].wait_recv()
            forward(m, g)

    def project(k, block, first=False):
        lo, hi = k[0] * per, k[1] * per
        x = xbuf[block, pl.ds(lo, hi - lo)].astype(F32).reshape((hi - lo) * cap, feats).astype(BF16)
        at = cols_of(block)
        to = pl.ds(lo * cap, (hi - lo) * cap)
        if first:
            gacc[to, :] = mt(x, eg[:, at])
            uacc[to, :] = mt(x, eu[:, at])
        else:
            gacc[to, :] += mt(x, eg[:, at])
            uacc[to, :] += mt(x, eu[:, at])

    def forwarded(k, m):
        for g in range(*k):
            if (m, g) in forwards:
                forwards[m, g].wait_recv()

    def project_near(k):
        project(k, t, True)
        forwarded(k, 0)
        project(k, block_of(0, 1 - c))

    def project_own(k):
        for m in range(1, ny):
            project(k, block_of(m, c))

    def project_last(k):
        for m in range(1, ny):
            forwarded(k, m)
            project(k, block_of(m, 1 - c))

    def out_cols(m, core):
        return cols_of(lax.rem(y + m, ny) * 2 + core)

    down_x, down_y, returns = {}, {}, []
    order = list(range(1, ny)) + [0]

    def down(k):
        i = chunks.index(k)
        lo, hi = k[0] * per, k[1] * per
        to = pl.ds(lo * cap, (hi - lo) * cap)
        at = pl.ds(lo, hi - lo)
        hid = (jax.nn.silu(gacc[to, :]) * uacc[to, :]).astype(BF16)
        for m in order:
            down_s[m, at] = mm(hid, ed[:, out_cols(m, 1 - c)]).reshape(hi - lo, cap, feats).astype(BF16)
            copy = remote(down_s.at[m, at], down_r.at[m, at], dp_ss.at[m, i], dp_rs.at[m, i], partner)
            copy.start()
            down_x[m, i] = copy
            down_m[m, at] = mm(hid, ed[:, out_cols(m, c)]).reshape(hi - lo, cap, feats)

    def cross(k):
        i = chunks.index(k)
        for m in order[:-1]:
            down_x[m, i].wait_recv()
        for g in range(*k):
            at = pl.ds(g * per, per)
            for m in order[:-1]:
                pair[m, at] = (down_m[m, at] + down_r[m, at].astype(F32)).astype(BF16)
                copy = remote(pair.at[m, at], yrecv.at[m, at], dy_ss.at[m, g], dy_rs.at[m, g], y_peer(m))
                copy.start()
                down_y[m, g] = copy
        down_x[0, i].wait_recv()

    def give_back(*gs):
        for g in gs:
            at = pl.ds(g * per, per)
            summed = down_m[0, at] + down_r[0, at].astype(F32)
            for m in range(1, ny):
                down_y[m, g].wait_recv()
                summed = summed + yrecv[m, at].astype(F32)
            ret_s[at] = summed.astype(BF16)
            for d in range(g * per, (g + 1) * per):
                if d == 0:
                    ret_r[0] = summed[0].astype(BF16)
                else:
                    copy = remote(ret_s.at[d], ret_r.at[d], rt_ss.at[d], rt_rs.at[d], ep_peer(d))
                    copy.start()
                    returns.append(copy)

    local["tok_a"].wait()
    local["gain_a"].wait()
    whole = tok_a[...].astype(F32)
    scale = lax.rsqrt(jnp.mean(whole * whole, axis=1, keepdims=True) + 1e-06)
    normed = (whole * scale * gain_a[...]).astype(BF16)
    local["val"].wait()
    value = mm(normed, val_w[...])
    local["gat"].wait()
    glu = (value * jax.nn.sigmoid(mm(normed, gat_w[...]))).astype(BF16)
    length = glu.shape[0]
    tail[...] = glu[length - HALO:]
    rim = remote(tail, halo, one_ss.at[0], one_rs.at[0], (lax.rem(e + 1, n), t))
    rim.start()
    dispatch(k3)
    pad[HALO:] = glu.astype(F32)

    local["eg"].wait()
    local["eu"].wait()
    if per > 1:
        arrive(0)
        hand_on(0)
    project_near(k0)
    project_own(k0)
    project_last(k0)
    local["ed"].wait()
    down(k0)
    arrive(6)
    arrive(1)
    hand_on(1)
    arrive(7)
    arrive(2)
    arrive(3)
    cross(k0)
    project_near(k2)

    local["taps"].wait()
    rim.wait_recv()
    pad[:HALO] = jnp.where(e > 0, halo[...].astype(F32), 0.0)
    width = taps.shape[0]
    chunk = min(128, pad.shape[1])
    total = jnp.zeros((length, 1), F32)
    square = jnp.zeros((length, 1), F32)
    mixed = []
    for lane in range(0, pad.shape[1], chunk):
        acc = jnp.zeros((length, chunk), F32)
        for tap in range(width):
            at = HALO - width + 1 + tap
            acc = acc + taps[tap:tap + 1, lane:lane + chunk] * pad[at:at + length, lane:lane + chunk]
        total = total + jnp.sum(acc, axis=1, keepdims=True)
        square = square + jnp.sum(acc * acc, axis=1, keepdims=True)
        mixed.append(acc)
    mixed = jnp.concatenate(mixed, axis=1)
    lanes = lax.broadcasted_iota(jnp.int32, (length, 128), 1)
    stats = jnp.where(lanes < 4, total, square).T
    st_s[...] = stats[0:8]
    stat = remote(st_s, st_r, one_ss.at[1], one_rs.at[1], partner)
    stat.start()

    hand_on(6)
    hand_on(7)
    project_own(k2)
    hand_on(2)
    project_last(k2)
    hand_on(3)
    down(k2)
    arrive(4)
    stat.wait_recv()
    st_ys[...] = st_s[...] + st_r[...]
    stat_y = []
    for m in range(1, ny):
        copy = remote(st_ys, st_yr.at[m], sy_ss.at[m], sy_rs.at[m], y_peer(m))
        copy.start()
        stat_y.append(copy)
    arrive(5)
    cross(k2)
    project_near(k1)
    project_own(k1)
    hand_on(4)
    project_last(k1)
    project_near(k3)
    hand_on(5)
    project_own(k3)
    give_back(6)
    project_last(k3)
    down(k3)
    give_back(7)
    cross(k3)
    down(k1)

    sums = st_ys[...]
    for m in range(1, ny):
        stat_y[m - 1].wait_recv()
        sums = sums + st_yr[m]
    local["chan"].wait()
    local["out"].wait()
    back = jnp.concatenate([sums] * (length // 8), axis=0).T
    average = back[:, 0:1] / channels
    spread = back[:, 4:5] / channels - average * average
    act = jax.nn.silu((mixed - average) * lax.rsqrt(spread + 1e-05) * chan_gain[...]).astype(BF16)

    conv_x = []
    for m in range(ny):
        conv_s[m] = mm(act, out_w[:, out_cols(m, 1 - c)]).astype(BF16)
        copy = remote(conv_s.at[m], conv_r.at[m], cp_ss.at[m], cp_rs.at[m], partner)
        copy.start()
        conv_x.append(copy)
        conv_m[m] = mm(act, out_w[:, out_cols(m, c)])

    cross(k1)
    give_back(4)

    conv_cross = []
    for m in range(ny):
        conv_x[m].wait_recv()
        summed = conv_m[m] + conv_r[m].astype(F32)
        if m == 0:
            conv_m[0] = summed
        else:
            conv_p[m] = summed.astype(BF16)
            copy = remote(conv_p.at[m], conv_y.at[m], cy_ss.at[m], cy_rs.at[m], y_peer(m))
            copy.start()
            conv_cross.append(copy)

    give_back(5)
    give_back(0, 1)

    local["logits"].wait()
    logit = logits[...]
    top = jnp.max(logit, axis=0, keepdims=True)
    exps = jnp.exp(logit - top)
    weight = exps / jnp.sum(exps, axis=0, keepdims=True)
    weight0, weight1 = upright(weight[0:1]), upright(weight[1:2])
    slots = lax.broadcasted_iota(jnp.int32, (count, rows), 1).astype(F32)
    combine = jnp.where(slots == slot0, weight0, 0.0) + jnp.where(slots == slot1, weight1, 0.0)
    high = combine.astype(BF16)
    low = (combine - high.astype(F32)).astype(BF16)
    give_back(2, 3)

    result = conv_m[0]
    for m in range(1, ny):
        conv_cross[m - 1].wait_recv()
        result = result + conv_y[m].astype(F32)
    conv_o[...] = result.astype(BF16)

    for copy in returns:
        copy.wait_recv()
    returned = ret_r[...].astype(F32).reshape(rows, feats).astype(BF16)
    moe_o[...] = (mm(high, returned) + mm(low, returned)).astype(BF16)

    sent = list(a2a.values()) + list(nears.values()) + list(crossings.values()) + list(forwards.values())
    sent += [rim, stat] + stat_y + conv_x + conv_cross
    sent += list(down_x.values()) + list(down_y.values()) + returns
    for copy in sent:
        copy.wait_send()


def solution(mesh):
    n = mesh.shape["ep"]
    n_tp = mesh.shape["tp"]
    ny = n_tp // 2
    groups = 8
    if n % groups or n & (n - 1):
        raise ValueError("ep size")
    near_groups = 2 if n == groups else 1
    chunks = [(0, 1), (1, 4), (6, 8), (4, 6)]

    def body(tokens_a, gain_a, value_w, gate_w, kernel, chan_gain, out_w,
             tokens_b, gain_b, routes, logits, eg, eu, ed):
        len_a, model = tokens_a.shape
        len_b = tokens_b.shape[0]
        chans = value_w.shape[1]
        feats = model // n_tp
        hidden = eg.shape[2]
        cap = 3 * len_b * routes.shape[1] // (2 * n)
        cap = -(-cap // 8) * 8
        rows = n * cap
        topk = routes.shape[1]
        near = near_groups * n // groups
        dma = pltpu.SemaphoreType.DMA
        vmem = pltpu.VMEM
        blocks = (n, cap, feats)
        scratch = [
            vmem((len_a, model), BF16), vmem((len_b, model), BF16),
            vmem((model, chans), BF16), vmem((model, chans), BF16), vmem((chans, model), BF16),
            vmem((hidden, model), BF16), vmem((hidden, model), BF16), vmem((hidden, model), BF16),
            vmem((1, model), F32), vmem((1, model), F32), vmem(kernel.shape, F32), vmem((1, chans), F32),
            vmem((topk, len_b), jnp.int32), vmem((topk, len_b), F32),
            vmem(blocks, BF16), vmem((ny, near, cap, feats), BF16), vmem((n_tp,) + blocks, BF16),
            vmem((rows, hidden), F32), vmem((rows, hidden), F32),
            vmem((ny,) + blocks, BF16), vmem((ny,) + blocks, BF16), vmem((ny,) + blocks, F32),
            vmem((ny,) + blocks, BF16), vmem((ny,) + blocks, BF16),
            vmem(blocks, BF16), vmem(blocks, BF16),
            vmem((HALO + len_a, chans), F32), vmem((HALO, chans), BF16), vmem((HALO, chans), BF16),
            vmem((8, len_a), F32), vmem((8, len_a), F32), vmem((8, len_a), F32), vmem((ny, 8, len_a), F32),
            vmem((ny, len_a, feats), BF16), vmem((ny, len_a, feats), BF16), vmem((ny, len_a, feats), F32),
            vmem((ny, len_a, feats), BF16), vmem((ny, len_a, feats), BF16),
            dma((14,)), dma((n,)), dma((n,)), dma((ny, near)), dma((ny, near)),
            dma((ny, groups)), dma((ny, groups)), dma((ny, groups)), dma((ny, groups)),
            dma((ny, 4)), dma((ny, 4)), dma((ny, groups)), dma((ny, groups)), dma((n,)), dma((n,)),
            dma((2,)), dma((2,)),
            dma((ny,)), dma((ny,)), dma((ny,)), dma((ny,)), dma((ny,)), dma((ny,)),
        ]
        hbm = pl.BlockSpec(memory_space=pl.ANY)
        here = pl.BlockSpec(memory_space=vmem)
        conv, moe = pl.pallas_call(
            functools.partial(kernel_body, n, ny, cap, groups, near_groups, chunks, chans * n_tp),
            out_shape=(
                vmem((len_a, feats), BF16),
                vmem((len_b, feats), BF16),
            ),
            in_specs=[hbm] * 14,
            out_specs=(here, here),
            scratch_shapes=scratch,
            compiler_params=pltpu.CompilerParams(
                collective_id=0, has_side_effects=True, vmem_limit_bytes=62914560
            ),
        )(tokens_a, gain_a[None, :], value_w, gate_w, kernel, chan_gain[None, :], out_w,
          tokens_b, gain_b[None, :], routes.T, logits.T, eg.swapaxes(1, 2), eu.swapaxes(1, 2), ed)

        def finish(conv_i, moe_i, conv_f, moe_f):
            conv_f[...] = conv_i[...].T
            moe_f[...] = moe_i[...]

        conv, moe = pl.pallas_call(
            finish,
            out_shape=(
                jax.ShapeDtypeStruct((feats, len_a), BF16),
                jax.ShapeDtypeStruct((len_b, feats), BF16),
            ),
            in_specs=[here, here],
            out_specs=(here, here),
            compiler_params=pltpu.CompilerParams(vmem_limit_bytes=4 * 1024 * 1024),
        )(conv, moe)
        return conv, moe.T

    return jax.shard_map(
        body,
        mesh=mesh,
        in_specs=(
            P("ep", None), P(), P(None, "tp"), P(None, "tp"), P(None, "tp"), P("tp"), P("tp", None),
            P("ep", None), P(), P("ep", None), P("ep", None),
            P("ep", None, "tp"), P("ep", None, "tp"), P("ep", "tp", None),
        ),
        out_specs=(P("tp", "ep"), P("tp", "ep")),
        check_vma=False,
    )
```

```python
import functools

import jax
import jax.numpy as jnp
from jax import lax
from jax.experimental import pallas as pl
from jax.experimental.pallas import tpu as pltpu
from jax.sharding import PartitionSpec as P

MESH = pl.DeviceIdType.MESH
F32 = jnp.float32
BF16 = jnp.bfloat16
HALO = 32


def mm(a, b):
    return jnp.dot(a, b, preferred_element_type=F32)


def mt(a, b):
    return lax.dot_general(a, b, (((1,), (1,)), ((), ())), preferred_element_type=F32)


def kernel_body(
    n, ny, cap, groups, near_groups, chunks, channels,
    tokens_a_h, gain_a_h, value_h, gate_h, taps_h, chan_gain_h, out_h,
    tokens_b_h, gain_b_h, routes_h, logits_h, eg_h, eu_h, ed_h,
    conv_o, moe_o,
    tok_a, tok_b, val_w, gat_w, out_w, eg, eu, ed, gain_a, gain_b, taps, chan_gain, routes, logits,
    send, nsend, xbuf, gacc, uacc, down_s, down_r, down_m, pair, yrecv, ret_s, ret_r,
    pad, mix, tail, halo, st_s, st_r, st_ys, st_yr, conv_s, conv_r, conv_m, conv_p, conv_y,
    loc, out_sem, a2a_rs, nr_rs, fw_rs, ya_rs, dp_rs, dy_rs, rt_rs, one_rs, sy_rs, cp_rs, cy_rs,
):
    e = lax.axis_index("ep")
    t = lax.axis_index("tp")
    y = t // 2
    c = t % 2
    partner = (e, y * 2 + (1 - c))
    feats = xbuf.shape[3]
    rows = n * cap
    per = n // groups
    near = near_groups * per

    def flip(v, d):
        bit = 1
        while bit <= d:
            if d & bit:
                v = v + bit - 2 * bit * lax.rem(v // bit, 2)
            bit *= 2
        return v

    def ep_peer(d):
        return (flip(e, d), t)

    def y_peer(m):
        return (e, lax.rem(y + m, ny) * 2 + c)

    def block_of(m, core):
        return lax.rem(y + ny - m, ny) * 2 + core

    def cols_of(block):
        return pl.ds(pl.multiple_of(block * feats, feats), feats)

    def remote(src, dst, rs, device):
        return pltpu.make_async_remote_copy(
            src_ref=src, dst_ref=dst, send_sem=out_sem.at[0], recv_sem=rs, device_id=device, device_id_type=MESH
        )

    pairs = dict(
        routes=(routes_h, routes), tok_b=(tokens_b_h, tok_b), gain_b=(gain_b_h, gain_b),
        tok_a=(tokens_a_h, tok_a), gain_a=(gain_a_h, gain_a), val=(value_h, val_w), gat=(gate_h, gat_w),
        taps=(taps_h, taps), eg=(eg_h.at[0], eg), eu=(eu_h.at[0], eu), ed=(ed_h.at[0], ed),
        chan=(chan_gain_h, chan_gain), out=(out_h, out_w), logits=(logits_h, logits),
    )
    local = {
        name: pltpu.make_async_copy(src, dst, loc.at[i]) for i, (name, (src, dst)) in enumerate(pairs.items())
    }
    for name in ("routes", "tok_b", "gain_b"):
        local[name].start()

    barrier = pltpu.get_barrier_semaphore()
    for d in range(n - 1, 0, -1):
        pl.semaphore_signal(barrier, inc=1, device_id=ep_peer(d), device_id_type=MESH)
    pl.semaphore_signal(barrier, inc=1, device_id=partner, device_id_type=MESH)
    for m in range(1, ny):
        pl.semaphore_signal(barrier, inc=1, device_id=y_peer(m), device_id_type=MESH)
    for name in list(pairs)[3:]:
        local[name].start()

    count = tok_b.shape[0]
    row = lax.broadcasted_iota(jnp.int32, (count, count), 0)
    col = lax.broadcasted_iota(jnp.int32, (count, count), 1)

    def upright(line):
        return jnp.sum(jnp.where(row == col, line, 0.0), axis=1, keepdims=True)

    local["routes"].wait()
    rel = jnp.bitwise_xor(routes[...], e).astype(F32)
    rel0, rel1 = upright(rel[0:1]), upright(rel[1:2])
    expert = lax.broadcasted_iota(jnp.int32, (count, n), 1).astype(F32)
    is0, is1 = expert == rel0, expert == rel1
    named = (jnp.where(is0, 1.0, 0.0) + jnp.where(is1, 1.0, 0.0)).astype(BF16)
    before = mm(jnp.where(row > col, 1.0, 0.0).astype(BF16), named)
    slot0 = rel0 * cap + jnp.sum(jnp.where(is0, before, 0.0), axis=1, keepdims=True)
    slot1 = rel1 * cap + jnp.sum(jnp.where(is1, before, 0.0), axis=1, keepdims=True)
    across0 = jnp.sum(jnp.where(row == col, slot0, 0.0), axis=0, keepdims=True)
    across1 = jnp.sum(jnp.where(row == col, slot1, 0.0), axis=0, keepdims=True)

    def picker(lo, hi):
        ids = lax.broadcasted_iota(jnp.int32, ((hi - lo) * cap, count), 0).astype(F32) + lo * cap
        return jnp.where((ids == across0) | (ids == across1), 1.0, 0.0).astype(BF16)

    local["tok_b"].wait()
    local["gain_b"].wait()
    whole = tok_b[...].astype(F32)
    scale_b = lax.rsqrt(jnp.mean(whole * whole, axis=1, keepdims=True) + 1e-06)

    def normed_b(block):
        at = cols_of(block)
        return (tok_b[:, at].astype(F32) * scale_b * gain_b[:, at]).astype(BF16)

    k0, k1, k2, k3 = chunks
    own = normed_b(t)

    def pick(lo, hi):
        send[lo:hi] = mm(picker(lo, hi), own).reshape(hi - lo, cap, feats).astype(BF16)

    pick(k2[0] * per, k2[1] * per)
    pl.semaphore_wait(barrier, n + ny - 1)
    a2a, nears, crossings, forwards = {}, {}, {}, {}

    def dispatch(k):
        for d in range(max(1, k[0] * per), k[1] * per):
            a2a[d] = remote(send.at[d], xbuf.at[t, d], a2a_rs.at[d], ep_peer(d))
            a2a[d].start()

    dispatch(k2)
    pick(0, k2[0] * per)
    dispatch(k0)
    dispatch(k1)
    xbuf[t, 0] = send[0]

    pick_near, pick_own = picker(0, near), picker(0, 1)
    for m in range(1, ny):
        block = block_of(m, c)
        picked = mm(pick_near, normed_b(block)).reshape(near, cap, feats).astype(BF16)
        nsend[m] = picked
        xbuf[block, 0] = picked[0]

    def second(k):
        for m in range(1, ny):
            for d in range(max(1, k[0] * per), k[1] * per):
                to = xbuf.at[block_of(m, c), d]
                copy = remote(nsend.at[m, d], to, nr_rs.at[m - 1, d], ep_peer(d))
                copy.start()
                nears[m, d] = copy

    second(k0)
    for m in range(ny):
        block = block_of(m, 1 - c)
        xbuf[block, 0] = mm(pick_own, normed_b(block)).astype(BF16)

    def span(g):
        return max(1, g * per), (g + 1) * per

    def forward(m, g):
        lo, hi = span(g)
        if lo < hi:
            part = xbuf.at[block_of(m, c), pl.ds(lo, hi - lo)]
            copy = remote(part, part, fw_rs.at[m, g], partner)
            copy.start()
            forwards[m, g] = copy

    def arrive(g):
        lo, hi = span(g)
        for d in range(lo, hi):
            a2a[d].wait_recv()
        if g >= near_groups:
            part = xbuf.at[t, pl.ds(lo, hi - lo)]
            for m in range(1, ny):
                copy = remote(part, part, ya_rs.at[m - 1, g - near_groups], y_peer(m))
                copy.start()
                crossings[m, g] = copy
        forward(0, g)

    def hand_on(g):
        for m in range(1, ny):
            if g >= near_groups:
                crossings[m, g].wait_recv()
            else:
                for d in range(*span(g)):
                    nears[m, d].wait_recv()
            forward(m, g)

    def project(k, block, first=False):
        lo, hi = k[0] * per, k[1] * per
        x = xbuf[block, pl.ds(lo, hi - lo)].astype(F32).reshape((hi - lo) * cap, feats).astype(BF16)
        at = cols_of(block)
        to = pl.ds(lo * cap, (hi - lo) * cap)
        if first:
            gacc[to, :] = mt(x, eg[:, at])
            uacc[to, :] = mt(x, eu[:, at])
        else:
            gacc[to, :] += mt(x, eg[:, at])
            uacc[to, :] += mt(x, eu[:, at])

    def forwarded(k, m):
        for g in range(*k):
            if (m, g) in forwards:
                forwards[m, g].wait_recv()

    def project_other(k):
        forwarded(k, 0)
        project(k, block_of(0, 1 - c))

    def project_near(k):
        project(k, t, True)
        project_other(k)

    def project_own(k):
        for m in range(1, ny):
            project(k, block_of(m, c))

    def project_last(k):
        for m in range(1, ny):
            forwarded(k, m)
            project(k, block_of(m, 1 - c))

    def out_cols(m, core):
        return cols_of(lax.rem(y + m, ny) * 2 + core)

    down_x, down_y, returns = {}, {}, {}
    order = list(range(1, ny)) + [0]

    def down(k):
        i = chunks.index(k)
        lo, hi = k[0] * per, k[1] * per
        to = pl.ds(lo * cap, (hi - lo) * cap)
        at = pl.ds(lo, hi - lo)
        hid = (jax.nn.silu(gacc[to, :]) * uacc[to, :]).astype(BF16)
        for m in order:
            down_s[m, at] = mm(hid, ed[:, out_cols(m, 1 - c)]).reshape(hi - lo, cap, feats).astype(BF16)
            copy = remote(down_s.at[m, at], down_r.at[m, at], dp_rs.at[m, i], partner)
            copy.start()
            down_x[m, i] = copy
            down_m[m, at] = mm(hid, ed[:, out_cols(m, c)]).reshape(hi - lo, cap, feats)

    def cross(k):
        i = chunks.index(k)
        for m in order[:-1]:
            down_x[m, i].wait_recv()
        for g in range(*k):
            at = pl.ds(g * per, per)
            for m in order[:-1]:
                pair[m, at] = (down_m[m, at] + down_r[m, at].astype(F32)).astype(BF16)
                copy = remote(pair.at[m, at], yrecv.at[m, at], dy_rs.at[m - 1, g], y_peer(m))
                copy.start()
                down_y[m, g] = copy
        down_x[0, i].wait_recv()

    def give_back(*gs):
        for g in gs:
            at = pl.ds(g * per, per)
            summed = down_m[0, at] + down_r[0, at].astype(F32)
            for m in range(1, ny):
                down_y[m, g].wait_recv()
                summed = summed + yrecv[m, at].astype(F32)
            ret_s[at] = summed.astype(BF16)
            for d in range(g * per, (g + 1) * per):
                if d == 0:
                    ret_r[0] = summed[0].astype(BF16)
                else:
                    copy = remote(ret_s.at[d], ret_r.at[d], rt_rs.at[d], ep_peer(d))
                    copy.start()
                    returns[d] = copy

    local["tok_a"].wait()
    local["gain_a"].wait()
    whole = tok_a[...].astype(F32)
    scale = lax.rsqrt(jnp.mean(whole * whole, axis=1, keepdims=True) + 1e-06)
    normed = (whole * scale * gain_a[...]).astype(BF16)
    local["val"].wait()
    value = mm(normed, val_w[...])
    local["gat"].wait()
    glu = (value * jax.nn.sigmoid(mm(normed, gat_w[...]))).astype(BF16)
    length = glu.shape[0]
    tail[...] = glu[length - HALO:]
    rim = remote(tail, halo, one_rs.at[0], (lax.rem(e + 1, n), t))
    rim.start()
    dispatch(k3)
    second(k1)
    pad[HALO:] = glu.astype(F32)

    local["taps"].wait()
    width = taps.shape[0]
    chunk = min(128, pad.shape[1])

    def convolve(first, last):
        total = jnp.zeros((last - first, 1), F32)
        square = jnp.zeros((last - first, 1), F32)
        for lane in range(0, pad.shape[1], chunk):
            acc = jnp.zeros((last - first, chunk), F32)
            for tap in range(width):
                at = HALO - width + 1 + tap
                acc = acc + taps[tap:tap + 1, lane:lane + chunk] * pad[at + first:at + last, lane:lane + chunk]
            total = total + jnp.sum(acc, axis=1, keepdims=True)
            square = square + jnp.sum(acc * acc, axis=1, keepdims=True)
            mix[first:last, lane:lane + chunk] = acc
        return total, square

    rest_total, rest_square = convolve(HALO, length)

    local["eg"].wait()
    local["eu"].wait()
    if per > 1:
        arrive(0)
        hand_on(0)
    arrive(1)
    project(k0, t, True)
    hand_on(1)
    project_own(k0)
    arrive(6)
    project_other(k0)
    project_last(k0)
    arrive(7)
    local["ed"].wait()
    down(k0)
    project(k2, t, True)
    cross(k0)
    arrive(2)
    arrive(3)
    project_other(k2)
    project(k1, t, True)

    rim.wait_recv()
    pad[:HALO] = jnp.where(e > 0, halo[...].astype(F32), 0.0)
    rim_total, rim_square = convolve(0, HALO)
    total = jnp.concatenate([rim_total, rest_total], axis=0)
    square = jnp.concatenate([rim_square, rest_square], axis=0)
    lanes = lax.broadcasted_iota(jnp.int32, (length, 128), 1)
    stats = jnp.where(lanes < 4, total, square).T
    st_s[...] = stats[0:8]
    stat = remote(st_s, st_r, one_rs.at[1], partner)
    stat.start()

    hand_on(6)
    hand_on(7)
    project_own(k2)
    stat.wait_recv()
    st_ys[...] = st_s[...] + st_r[...]
    stat_y = []
    for m in range(1, ny):
        copy = remote(st_ys, st_yr.at[m], sy_rs.at[m - 1], y_peer(m))
        copy.start()
        stat_y.append(copy)
    arrive(4)
    project_last(k2)
    arrive(5)
    hand_on(2)
    hand_on(3)
    down(k2)
    project_other(k1)
    cross(k2)
    give_back(0, 1)
    project_own(k1)
    project_last(k1)
    down(k1)
    hand_on(4)
    project(k3, t, True)
    project_other(k3)
    cross(k1)
    hand_on(5)
    project_own(k3)
    give_back(6)
    project_last(k3)
    down(k3)
    give_back(7)

    sums = st_ys[...]
    for m in range(1, ny):
        stat_y[m - 1].wait_recv()
        sums = sums + st_yr[m]
    local["chan"].wait()
    local["out"].wait()
    back = jnp.concatenate([sums] * (length // 8), axis=0).T
    average = back[:, 0:1] / channels
    spread = back[:, 4:5] / channels - average * average
    act = jax.nn.silu((mix[...] - average) * lax.rsqrt(spread + 1e-05) * chan_gain[...]).astype(BF16)

    conv_x = []
    for m in range(ny):
        conv_s[m] = mm(act, out_w[:, out_cols(m, 1 - c)]).astype(BF16)
        copy = remote(conv_s.at[m], conv_r.at[m], cp_rs.at[m], partner)
        copy.start()
        conv_x.append(copy)
        conv_m[m] = mm(act, out_w[:, out_cols(m, c)])

    cross(k3)
    give_back(2)
    give_back(3)

    conv_cross = []
    for m in range(ny):
        conv_x[m].wait_recv()
        summed = conv_m[m] + conv_r[m].astype(F32)
        if m == 0:
            conv_m[0] = summed
        else:
            conv_p[m] = summed.astype(BF16)
            copy = remote(conv_p.at[m], conv_y.at[m], cy_rs.at[m - 1], y_peer(m))
            copy.start()
            conv_cross.append(copy)

    local["logits"].wait()
    logit = logits[...]
    top = jnp.max(logit, axis=0, keepdims=True)
    exps = jnp.exp(logit - top)
    weight = exps / jnp.sum(exps, axis=0, keepdims=True)
    weight0, weight1 = upright(weight[0:1]), upright(weight[1:2])

    def combined(k):
        lo, hi = k[0] * per, k[1] * per
        slots = lax.broadcasted_iota(jnp.int32, (count, (hi - lo) * cap), 1).astype(F32) + lo * cap
        combine = jnp.where(slots == slot0, weight0, 0.0) + jnp.where(slots == slot1, weight1, 0.0)
        high = combine.astype(BF16)
        low = (combine - high.astype(F32)).astype(BF16)
        for d in range(max(1, lo), hi):
            returns[d].wait_recv()
        came = ret_r[lo:hi].astype(F32).reshape((hi - lo) * cap, feats).astype(BF16)
        return mm(high, came) + mm(low, came)

    give_back(4)
    moved = combined(k0)
    give_back(5)

    result = conv_m[0]
    for m in range(1, ny):
        conv_cross[m - 1].wait_recv()
        result = result + conv_y[m].astype(F32)
    conv_o[...] = result.astype(BF16)

    moved = moved + combined(k1)
    moved = moved + combined(k2)
    moe_o[...] = (moved + combined(k3)).astype(BF16)

    sent = list(a2a.values()) + list(nears.values()) + list(crossings.values()) + list(forwards.values())
    sent += [rim, stat] + stat_y + conv_x + conv_cross
    sent += list(down_x.values()) + list(down_y.values()) + list(returns.values())
    for copy in sent:
        copy.wait_send()


def solution(mesh):
    n = mesh.shape["ep"]
    n_tp = mesh.shape["tp"]
    ny = n_tp // 2
    groups = 8
    if n % groups or n & (n - 1):
        raise ValueError("ep size")
    near_groups = 4
    chunks = [(0, 2), (2, 4), (6, 8), (4, 6)]

    def body(tokens_a, gain_a, value_w, gate_w, kernel, chan_gain, out_w,
             tokens_b, gain_b, routes, logits, eg, eu, ed):
        len_a, model = tokens_a.shape
        len_b = tokens_b.shape[0]
        chans = value_w.shape[1]
        feats = model // n_tp
        hidden = eg.shape[2]
        cap = 3 * len_b * routes.shape[1] // (2 * n)
        cap = -(-cap // 8) * 8
        rows = n * cap
        topk = routes.shape[1]
        near = near_groups * n // groups
        dma = pltpu.SemaphoreType.DMA
        vmem = pltpu.VMEM
        blocks = (n, cap, feats)
        scratch = [
            vmem((len_a, model), BF16), vmem((len_b, model), BF16),
            vmem((model, chans), BF16), vmem((model, chans), BF16), vmem((chans, model), BF16),
            vmem((hidden, model), BF16), vmem((hidden, model), BF16), vmem((hidden, model), BF16),
            vmem((1, model), F32), vmem((1, model), F32), vmem(kernel.shape, F32), vmem((1, chans), F32),
            vmem((topk, len_b), jnp.int32), vmem((topk, len_b), F32),
            vmem(blocks, BF16), vmem((ny, near, cap, feats), BF16), vmem((n_tp,) + blocks, BF16),
            vmem((rows, hidden), F32), vmem((rows, hidden), F32),
            vmem((ny,) + blocks, BF16), vmem((ny,) + blocks, BF16), vmem((ny,) + blocks, F32),
            vmem((ny,) + blocks, BF16), vmem((ny,) + blocks, BF16),
            vmem(blocks, BF16), vmem(blocks, BF16),
            vmem((HALO + len_a, chans), F32), vmem((len_a, chans), F32), vmem((HALO, chans), BF16), vmem((HALO, chans), BF16),
            vmem((8, len_a), F32), vmem((8, len_a), F32), vmem((8, len_a), F32), vmem((ny, 8, len_a), F32),
            vmem((ny, len_a, feats), BF16), vmem((ny, len_a, feats), BF16), vmem((ny, len_a, feats), F32),
            vmem((ny, len_a, feats), BF16), vmem((ny, len_a, feats), BF16),
            dma((14,)), dma((1,)), dma((n,)), dma((ny - 1, near)), dma((ny, groups)),
            dma((ny - 1, groups - near_groups)), dma((ny, 4)), dma((ny - 1, groups)), dma((n,)),
            dma((2,)), dma((ny - 1,)), dma((ny,)), dma((ny - 1,)),
        ]
        hbm = pl.BlockSpec(memory_space=pl.ANY)
        here = pl.BlockSpec(memory_space=vmem)
        conv, moe = pl.pallas_call(
            functools.partial(kernel_body, n, ny, cap, groups, near_groups, chunks, chans * n_tp),
            out_shape=(
                vmem((len_a, feats), BF16),
                vmem((len_b, feats), BF16),
            ),
            in_specs=[hbm] * 14,
            out_specs=(here, here),
            scratch_shapes=scratch,
            compiler_params=pltpu.CompilerParams(
                collective_id=0, has_side_effects=True, vmem_limit_bytes=62914560
            ),
        )(tokens_a, gain_a[None, :], value_w, gate_w, kernel, chan_gain[None, :], out_w,
          tokens_b, gain_b[None, :], routes.T, logits.T, eg.swapaxes(1, 2), eu.swapaxes(1, 2), ed)

        def finish(conv_i, moe_i, conv_f, moe_f):
            conv_f[...] = conv_i[...].T
            moe_f[...] = moe_i[...]

        conv, moe = pl.pallas_call(
            finish,
            out_shape=(
                jax.ShapeDtypeStruct((feats, len_a), BF16),
                jax.ShapeDtypeStruct((len_b, feats), BF16),
            ),
            in_specs=[here, here],
            out_specs=(here, here),
            compiler_params=pltpu.CompilerParams(vmem_limit_bytes=4 * 1024 * 1024),
        )(conv, moe)
        return conv, moe.T

    return jax.shard_map(
        body,
        mesh=mesh,
        in_specs=(
            P("ep", None), P(), P(None, "tp"), P(None, "tp"), P(None, "tp"), P("tp"), P("tp", None),
            P("ep", None), P(), P("ep", None), P("ep", None),
            P("ep", None, "tp"), P("ep", None, "tp"), P("ep", "tp", None),
        ),
        out_specs=(P("tp", "ep"), P("tp", "ep")),
        check_vma=False,
    )
```

```python
import functools

import jax
import jax.numpy as jnp
from jax import lax
from jax.experimental import pallas as pl
from jax.experimental.pallas import tpu as pltpu
from jax.sharding import PartitionSpec as P

MESH = pl.DeviceIdType.MESH
F32 = jnp.float32
BF16 = jnp.bfloat16
HALO = 32


def mm(a, b):
    return jnp.dot(a, b, preferred_element_type=F32)


def mt(a, b):
    return lax.dot_general(a, b, (((1,), (1,)), ((), ())), preferred_element_type=F32)


def kernel_body(
    n, ny, cap, groups, near_groups, chunks, channels,
    tokens_a_h, gain_a_h, value_h, gate_h, taps_h, chan_gain_h, out_h,
    tokens_b_h, gain_b_h, routes_h, logits_h, eg_h, eu_h, ed_h,
    conv_o, moe_o,
    tok_a, tok_b, val_w, gat_w, out_w, eg, eu, ed, gain_a, gain_b, taps, chan_gain, routes, logits,
    send, nsend, xbuf, gacc, uacc, down_s, down_r, down_m, pair, yrecv, ret_s, ret_r,
    pad, mix, tail, halo, st_s, st_r, st_ys, st_yr, conv_s, conv_r, conv_m, conv_p, conv_y,
    loc, out_sem, a2a_rs, nr_rs, fw_rs, ya_rs, dp_rs, dy_rs, rt_rs, one_rs, sy_rs, cp_rs, cy_rs,
):
    e = lax.axis_index("ep")
    t = lax.axis_index("tp")
    y = t // 2
    c = t % 2
    partner = (e, y * 2 + (1 - c))
    feats = xbuf.shape[3]
    rows = n * cap
    per = n // groups
    near = near_groups * per

    def flip(v, d):
        bit = 1
        while bit <= d:
            if d & bit:
                v = v + bit - 2 * bit * lax.rem(v // bit, 2)
            bit *= 2
        return v

    def ep_peer(d):
        return (flip(e, d), t)

    def y_peer(m):
        return (e, lax.rem(y + m, ny) * 2 + c)

    def block_of(m, core):
        return lax.rem(y + ny - m, ny) * 2 + core

    def cols_of(block):
        return pl.ds(pl.multiple_of(block * feats, feats), feats)

    def remote(src, dst, rs, device):
        return pltpu.make_async_remote_copy(
            src_ref=src, dst_ref=dst, send_sem=out_sem.at[0], recv_sem=rs, device_id=device, device_id_type=MESH
        )

    pairs = dict(
        routes=(routes_h, routes), tok_b=(tokens_b_h, tok_b), gain_b=(gain_b_h, gain_b),
        tok_a=(tokens_a_h, tok_a), gain_a=(gain_a_h, gain_a), val=(value_h, val_w), gat=(gate_h, gat_w),
        taps=(taps_h, taps), eg=(eg_h.at[0], eg), eu=(eu_h.at[0], eu), ed=(ed_h.at[0], ed),
        chan=(chan_gain_h, chan_gain), out=(out_h, out_w), logits=(logits_h, logits),
    )
    local = {
        name: pltpu.make_async_copy(src, dst, loc.at[i]) for i, (name, (src, dst)) in enumerate(pairs.items())
    }
    for name in ("routes", "tok_b", "gain_b"):
        local[name].start()

    barrier = pltpu.get_barrier_semaphore()
    for d in range(n - 1, 0, -1):
        pl.semaphore_signal(barrier, inc=1, device_id=ep_peer(d), device_id_type=MESH)
    pl.semaphore_signal(barrier, inc=1, device_id=partner, device_id_type=MESH)
    for m in range(1, ny):
        pl.semaphore_signal(barrier, inc=1, device_id=y_peer(m), device_id_type=MESH)
    for name in list(pairs)[3:]:
        local[name].start()

    count = tok_b.shape[0]
    row = lax.broadcasted_iota(jnp.int32, (count, count), 0)
    col = lax.broadcasted_iota(jnp.int32, (count, count), 1)

    def upright(line):
        return jnp.sum(jnp.where(row == col, line, 0.0), axis=1, keepdims=True)

    local["routes"].wait()
    rel = jnp.bitwise_xor(routes[...], e).astype(F32)
    rel0, rel1 = upright(rel[0:1]), upright(rel[1:2])
    expert = lax.broadcasted_iota(jnp.int32, (count, n), 1).astype(F32)
    is0, is1 = expert == rel0, expert == rel1
    named = (jnp.where(is0, 1.0, 0.0) + jnp.where(is1, 1.0, 0.0)).astype(BF16)
    before = mm(jnp.where(row > col, 1.0, 0.0).astype(BF16), named)
    slot0 = rel0 * cap + jnp.sum(jnp.where(is0, before, 0.0), axis=1, keepdims=True)
    slot1 = rel1 * cap + jnp.sum(jnp.where(is1, before, 0.0), axis=1, keepdims=True)
    across0 = jnp.sum(jnp.where(row == col, slot0, 0.0), axis=0, keepdims=True)
    across1 = jnp.sum(jnp.where(row == col, slot1, 0.0), axis=0, keepdims=True)

    def picker(lo, hi):
        ids = lax.broadcasted_iota(jnp.int32, ((hi - lo) * cap, count), 0).astype(F32) + lo * cap
        return jnp.where((ids == across0) | (ids == across1), 1.0, 0.0).astype(BF16)

    local["tok_b"].wait()
    local["gain_b"].wait()
    whole = tok_b[...].astype(F32)
    scale_b = lax.rsqrt(jnp.mean(whole * whole, axis=1, keepdims=True) + 1e-06)

    def normed_b(block):
        at = cols_of(block)
        return (tok_b[:, at].astype(F32) * scale_b * gain_b[:, at]).astype(BF16)

    k0, k1, k2, k3 = chunks
    own = normed_b(t)

    def pick(lo, hi):
        send[lo:hi] = mm(picker(lo, hi), own).reshape(hi - lo, cap, feats).astype(BF16)

    pick(0, k0[1] * per)
    pick(k2[0] * per, k2[1] * per)
    pl.semaphore_wait(barrier, n + ny - 1)
    a2a, nears, crossings, forwards = {}, {}, {}, {}

    def dispatch(k):
        ds = list(range(max(1, k[0] * per), k[1] * per))
        for d in ds[::-1] if k is k3 else ds:
            a2a[d] = remote(send.at[d], xbuf.at[t, d], a2a_rs.at[d], ep_peer(d))
            a2a[d].start()

    dispatch(k0)
    dispatch(k2)
    pick(k0[1] * per, k2[0] * per)
    dispatch(k1)
    xbuf[t, 0] = send[0]

    pick_near, pick_own = picker(0, near), picker(0, 1)
    for m in range(1, ny):
        block = block_of(m, c)
        picked = mm(pick_near, normed_b(block)).reshape(near, cap, feats).astype(BF16)
        nsend[m] = picked
        xbuf[block, 0] = picked[0]

    def second(k):
        for m in range(1, ny):
            for d in range(max(1, k[0] * per), k[1] * per):
                to = xbuf.at[block_of(m, c), d]
                copy = remote(nsend.at[m, d], to, nr_rs.at[m - 1, d], ep_peer(d))
                copy.start()
                nears[m, d] = copy

    second(k0)
    for m in range(ny):
        block = block_of(m, 1 - c)
        xbuf[block, 0] = mm(pick_own, normed_b(block)).astype(BF16)

    def span(g):
        return max(1, g * per), (g + 1) * per

    def forward(m, g):
        lo, hi = span(g)
        if lo < hi:
            part = xbuf.at[block_of(m, c), pl.ds(lo, hi - lo)]
            copy = remote(part, part, fw_rs.at[m, g], partner)
            copy.start()
            forwards[m, g] = copy

    def arrive(g):
        lo, hi = span(g)
        for d in range(lo, hi):
            a2a[d].wait_recv()
        if g >= near_groups:
            part = xbuf.at[t, pl.ds(lo, hi - lo)]
            for m in range(1, ny):
                copy = remote(part, part, ya_rs.at[m - 1, g - near_groups], y_peer(m))
                copy.start()
                crossings[m, g] = copy
        forward(0, g)

    def hand_on(g):
        for m in range(1, ny):
            if g >= near_groups:
                crossings[m, g].wait_recv()
            else:
                for d in range(*span(g)):
                    nears[m, d].wait_recv()
            forward(m, g)

    def rows_of(k, block):
        lo, hi = k[0] * per, k[1] * per
        return xbuf[block, pl.ds(lo, hi - lo)].astype(F32).reshape((hi - lo) * cap, feats).astype(BF16)

    def accumulate(k, x, at, first):
        to = pl.ds(k[0] * per * cap, (k[1] - k[0]) * per * cap)
        if first:
            gacc[to, :] = mt(x, eg[:, at])
            uacc[to, :] = mt(x, eu[:, at])
        else:
            gacc[to, :] += mt(x, eg[:, at])
            uacc[to, :] += mt(x, eu[:, at])

    def project(k, block, first=False):
        accumulate(k, rows_of(k, block), cols_of(block), first)

    def forwarded(k, m):
        for g in range(*k):
            if (m, g) in forwards:
                forwards[m, g].wait_recv()

    def project_other(k):
        forwarded(k, 0)
        project(k, block_of(0, 1 - c))

    def project_pair(k, m, first=False):
        forwarded(k, m)
        base = lax.rem(y + ny - m, ny) * 2
        x = jnp.concatenate([rows_of(k, base), rows_of(k, base + 1)], axis=1)
        accumulate(k, x, pl.ds(pl.multiple_of(base * feats, 2 * feats), 2 * feats), first)

    def project_far(k):
        for m in range(1, ny):
            project_pair(k, m)

    def project_own(k):
        for m in range(1, ny):
            project(k, block_of(m, c))

    def project_last(k):
        for m in range(1, ny):
            forwarded(k, m)
            project(k, block_of(m, 1 - c))

    def out_cols(m, core):
        return cols_of(lax.rem(y + m, ny) * 2 + core)

    down_x, down_y, returns = {}, {}, {}
    order = list(range(1, ny)) + [0]

    def down(k):
        i = chunks.index(k)
        lo, hi = k[0] * per, k[1] * per
        to = pl.ds(lo * cap, (hi - lo) * cap)
        at = pl.ds(lo, hi - lo)
        hid = (jax.nn.silu(gacc[to, :]) * uacc[to, :]).astype(BF16)

        def product(m, core):
            return mm(hid, ed[:, out_cols(m, core)]).reshape(hi - lo, cap, feats)

        def exchange(m):
            copy = remote(down_s.at[m, at], down_r.at[m, at], dp_rs.at[m, i], partner)
            copy.start()
            down_x[m, i] = copy

        for m in order[:-1]:
            down_s[m, at] = product(m, 1 - c).astype(BF16)
            exchange(m)
        for m in order[:-1]:
            down_m[m, at] = product(m, c)
        down_s[0, at] = product(0, 1 - c).astype(BF16)
        down_m[0, at] = product(0, c)
        exchange(0)

    def cross_wait(k):
        for m in order[:-1]:
            down_x[m, chunks.index(k)].wait_recv()

    def cross_one(g):
        at = pl.ds(g * per, per)
        for m in order[:-1]:
            pair[m, at] = (down_m[m, at] + down_r[m, at].astype(F32)).astype(BF16)
            copy = remote(pair.at[m, at], yrecv.at[m, at], dy_rs.at[m - 1, g], y_peer(m))
            copy.start()
            down_y[m, g] = copy

    def cross(k):
        cross_wait(k)
        for g in reversed(range(*k)):
            cross_one(g)

    settled = []

    def give_back(*gs):
        for g in gs:
            i = [k[0] <= g < k[1] for k in chunks].index(True)
            if i not in settled:
                down_x[0, i].wait_recv()
                settled.append(i)
            at = pl.ds(g * per, per)
            summed = down_m[0, at] + down_r[0, at].astype(F32)
            for m in range(1, ny):
                down_y[m, g].wait_recv()
                summed = summed + yrecv[m, at].astype(F32)
            ret_s[at] = summed.astype(BF16)
            for d in range(g * per, (g + 1) * per):
                if d == 0:
                    ret_r[0] = summed[0].astype(BF16)
                else:
                    copy = remote(ret_s.at[d], ret_r.at[d], rt_rs.at[d], ep_peer(d))
                    copy.start()
                    returns[d] = copy

    local["tok_a"].wait()
    local["gain_a"].wait()
    whole = tok_a[...].astype(F32)
    scale = lax.rsqrt(jnp.mean(whole * whole, axis=1, keepdims=True) + 1e-06)
    normed = (whole * scale * gain_a[...]).astype(BF16)
    local["val"].wait()
    value = mm(normed, val_w[...])
    local["gat"].wait()
    glu = (value * jax.nn.sigmoid(mm(normed, gat_w[...]))).astype(BF16)
    length = glu.shape[0]
    tail[...] = glu[length - HALO:]
    rim = remote(tail, halo, one_rs.at[0], (lax.rem(e + 1, n), t))
    rim.start()
    dispatch(k3)
    second(k1)
    pad[HALO:] = glu.astype(F32)

    local["taps"].wait()
    width = taps.shape[0]
    chunk = min(128, pad.shape[1])

    def convolve(first, last):
        total = jnp.zeros((last - first, 1), F32)
        square = jnp.zeros((last - first, 1), F32)
        for lane in range(0, pad.shape[1], chunk):
            acc = jnp.zeros((last - first, chunk), F32)
            for tap in range(width):
                at = HALO - width + 1 + tap
                acc = acc + taps[tap:tap + 1, lane:lane + chunk] * pad[at + first:at + last, lane:lane + chunk]
            total = total + jnp.sum(acc, axis=1, keepdims=True)
            square = square + jnp.sum(acc * acc, axis=1, keepdims=True)
            mix[first:last, lane:lane + chunk] = acc
        return total, square

    rest_total, rest_square = convolve(HALO, length)

    local["eg"].wait()
    local["eu"].wait()
    if per > 1:
        arrive(0)
        hand_on(0)
    arrive(1)
    project(k0, t, True)
    hand_on(1)
    project_own(k0)
    arrive(6)
    project_other(k0)
    project_last(k0)
    arrive(7)
    local["ed"].wait()
    down(k0)
    project(k2, t, True)
    cross(k0)
    arrive(2)
    arrive(3)
    project_other(k2)
    project(k1, t, True)

    rim.wait_recv()
    pad[:HALO] = jnp.where(e > 0, halo[...].astype(F32), 0.0)
    rim_total, rim_square = convolve(0, HALO)
    total = jnp.concatenate([rim_total, rest_total], axis=0)
    square = jnp.concatenate([rim_square, rest_square], axis=0)
    lanes = lax.broadcasted_iota(jnp.int32, (length, 128), 1)
    stats = jnp.where(lanes < 4, total, square).T
    st_s[...] = stats[0:8]
    stat = remote(st_s, st_r, one_rs.at[1], partner)
    stat.start()

    hand_on(6)
    hand_on(7)
    project_own(k2)
    stat.wait_recv()
    st_ys[...] = st_s[...] + st_r[...]
    stat_y = []
    for m in range(1, ny):
        copy = remote(st_ys, st_yr.at[m], sy_rs.at[m - 1], y_peer(m))
        copy.start()
        stat_y.append(copy)
    arrive(5)
    project_last(k2)
    arrive(4)
    hand_on(2)
    hand_on(3)
    down(k2)
    project_other(k1)
    cross(k2)
    give_back(1, 0)
    project_far(k1)
    down(k1)
    hand_on(5)
    project_pair(k3, 0, True)
    cross(k1)
    hand_on(4)
    project_own(k3)
    give_back(7)
    project_last(k3)
    down(k3)
    give_back(6)

    sums = st_ys[...]
    for m in range(1, ny):
        stat_y[m - 1].wait_recv()
        sums = sums + st_yr[m]
    local["chan"].wait()
    local["out"].wait()
    back = jnp.concatenate([sums] * (length // 8), axis=0).T
    average = back[:, 0:1] / channels
    spread = back[:, 4:5] / channels - average * average
    act = jax.nn.silu((mix[...] - average) * lax.rsqrt(spread + 1e-05) * chan_gain[...]).astype(BF16)

    cross(k3)

    conv_x = []
    for m in range(ny):
        conv_s[m] = mm(act, out_w[:, out_cols(m, 1 - c)]).astype(BF16)
        copy = remote(conv_s.at[m], conv_r.at[m], cp_rs.at[m], partner)
        copy.start()
        conv_x.append(copy)
        conv_m[m] = mm(act, out_w[:, out_cols(m, c)])

    give_back(3)
    give_back(2)

    conv_cross = []
    for m in range(ny):
        conv_x[m].wait_recv()
        summed = conv_m[m] + conv_r[m].astype(F32)
        if m == 0:
            conv_m[0] = summed
        else:
            conv_p[m] = summed.astype(BF16)
            copy = remote(conv_p.at[m], conv_y.at[m], cy_rs.at[m - 1], y_peer(m))
            copy.start()
            conv_cross.append(copy)

    local["logits"].wait()
    logit = logits[...]
    top = jnp.max(logit, axis=0, keepdims=True)
    exps = jnp.exp(logit - top)
    weight = exps / jnp.sum(exps, axis=0, keepdims=True)
    weight0, weight1 = upright(weight[0:1]), upright(weight[1:2])

    def combined(k):
        lo, hi = k[0] * per, k[1] * per
        slots = lax.broadcasted_iota(jnp.int32, (count, (hi - lo) * cap), 1).astype(F32) + lo * cap
        combine = jnp.where(slots == slot0, weight0, 0.0) + jnp.where(slots == slot1, weight1, 0.0)
        high = combine.astype(BF16)
        low = (combine - high.astype(F32)).astype(BF16)
        for d in range(max(1, lo), hi):
            returns[d].wait_recv()
        came = ret_r[lo:hi].astype(F32).reshape((hi - lo) * cap, feats).astype(BF16)
        return mm(high, came) + mm(low, came)

    give_back(5)
    moved = combined(k0)
    give_back(4)

    result = conv_m[0]
    for m in range(1, ny):
        conv_cross[m - 1].wait_recv()
        result = result + conv_y[m].astype(F32)
    conv_o[...] = result.astype(BF16)

    moved = moved + combined(k1)
    moved = moved + combined(k2)
    moe_o[...] = (moved + combined(k3)).astype(BF16)

    sent = list(a2a.values()) + list(nears.values()) + list(crossings.values()) + list(forwards.values())
    sent += [rim, stat] + stat_y + conv_x + conv_cross
    sent += list(down_x.values()) + list(down_y.values()) + list(returns.values())
    for copy in sent:
        copy.wait_send()


def solution(mesh):
    n = mesh.shape["ep"]
    n_tp = mesh.shape["tp"]
    ny = n_tp // 2
    groups = 8
    if n % groups or n & (n - 1):
        raise ValueError("ep size")
    near_groups = 4
    chunks = [(0, 2), (2, 4), (6, 8), (4, 6)]

    def body(tokens_a, gain_a, value_w, gate_w, kernel, chan_gain, out_w,
             tokens_b, gain_b, routes, logits, eg, eu, ed):
        len_a, model = tokens_a.shape
        len_b = tokens_b.shape[0]
        chans = value_w.shape[1]
        feats = model // n_tp
        hidden = eg.shape[2]
        cap = 3 * len_b * routes.shape[1] // (2 * n)
        cap = -(-cap // 8) * 8
        rows = n * cap
        topk = routes.shape[1]
        near = near_groups * n // groups
        dma = pltpu.SemaphoreType.DMA
        vmem = pltpu.VMEM
        blocks = (n, cap, feats)
        scratch = [
            vmem((len_a, model), BF16), vmem((len_b, model), BF16),
            vmem((model, chans), BF16), vmem((model, chans), BF16), vmem((chans, model), BF16),
            vmem((hidden, model), BF16), vmem((hidden, model), BF16), vmem((hidden, model), BF16),
            vmem((1, model), F32), vmem((1, model), F32), vmem(kernel.shape, F32), vmem((1, chans), F32),
            vmem((topk, len_b), jnp.int32), vmem((topk, len_b), F32),
            vmem(blocks, BF16), vmem((ny, near, cap, feats), BF16), vmem((n_tp,) + blocks, BF16),
            vmem((rows, hidden), F32), vmem((rows, hidden), F32),
            vmem((ny,) + blocks, BF16), vmem((ny,) + blocks, BF16), vmem((ny,) + blocks, F32),
            vmem((ny,) + blocks, BF16), vmem((ny,) + blocks, BF16),
            vmem(blocks, BF16), vmem(blocks, BF16),
            vmem((HALO + len_a, chans), F32), vmem((len_a, chans), F32), vmem((HALO, chans), BF16), vmem((HALO, chans), BF16),
            vmem((8, len_a), F32), vmem((8, len_a), F32), vmem((8, len_a), F32), vmem((ny, 8, len_a), F32),
            vmem((ny, len_a, feats), BF16), vmem((ny, len_a, feats), BF16), vmem((ny, len_a, feats), F32),
            vmem((ny, len_a, feats), BF16), vmem((ny, len_a, feats), BF16),
            dma((14,)), dma((1,)), dma((n,)), dma((ny - 1, near)), dma((ny, groups)),
            dma((ny - 1, groups - near_groups)), dma((ny, 4)), dma((ny - 1, groups)), dma((n,)),
            dma((2,)), dma((ny - 1,)), dma((ny,)), dma((ny - 1,)),
        ]
        hbm = pl.BlockSpec(memory_space=pl.ANY)
        here = pl.BlockSpec(memory_space=vmem)
        conv, moe = pl.pallas_call(
            functools.partial(kernel_body, n, ny, cap, groups, near_groups, chunks, chans * n_tp),
            out_shape=(
                vmem((len_a, feats), BF16),
                vmem((len_b, feats), BF16),
            ),
            in_specs=[hbm] * 14,
            out_specs=(here, here),
            scratch_shapes=scratch,
            compiler_params=pltpu.CompilerParams(
                collective_id=0, has_side_effects=True, vmem_limit_bytes=62914560
            ),
        )(tokens_a, gain_a[None, :], value_w, gate_w, kernel, chan_gain[None, :], out_w,
          tokens_b, gain_b[None, :], routes.T, logits.T, eg.swapaxes(1, 2), eu.swapaxes(1, 2), ed)

        def finish(conv_i, moe_i, conv_f, moe_f):
            conv_f[...] = conv_i[...].T
            moe_f[...] = moe_i[...]

        conv, moe = pl.pallas_call(
            finish,
            out_shape=(
                jax.ShapeDtypeStruct((feats, len_a), BF16),
                jax.ShapeDtypeStruct((len_b, feats), BF16),
            ),
            in_specs=[here, here],
            out_specs=(here, here),
            compiler_params=pltpu.CompilerParams(vmem_limit_bytes=4 * 1024 * 1024),
        )(conv, moe)
        return conv, moe.T

    return jax.shard_map(
        body,
        mesh=mesh,
        in_specs=(
            P("ep", None), P(), P(None, "tp"), P(None, "tp"), P(None, "tp"), P("tp"), P("tp", None),
            P("ep", None), P(), P("ep", None), P("ep", None),
            P("ep", None, "tp"), P("ep", None, "tp"), P("ep", "tp", None),
        ),
        out_specs=(P("tp", "ep"), P("tp", "ep")),
        check_vma=False,
    )
```

```python
import functools

import jax
import jax.numpy as jnp
from jax import lax
from jax.experimental import pallas as pl
from jax.experimental.pallas import tpu as pltpu
from jax.sharding import PartitionSpec as P

MESH = pl.DeviceIdType.MESH
F32 = jnp.float32
BF16 = jnp.bfloat16
HALO = 32


def mm(a, b):
    return jnp.dot(a, b, preferred_element_type=F32)


def mt(a, b):
    return lax.dot_general(a, b, (((1,), (1,)), ((), ())), preferred_element_type=F32)


def kernel_body(
    n, ny, cap, groups, near_groups, chunks, channels,
    tokens_a_h, gain_a_h, value_h, gate_h, taps_h, chan_gain_h, out_h,
    tokens_b_h, gain_b_h, routes_h, logits_h, eg_h, eu_h, ed_h,
    conv_o, moe_o,
    tok_a, tok_b, val_w, gat_w, out_w, eg, eu, ed, gain_a, gain_b, taps, chan_gain, routes, logits,
    send, nsend, xbuf, gacc, uacc, down_s, down_r, down_m, pair, yrecv, ret_s, ret_r,
    pad, mix, tail, halo, st_s, st_r, st_ys, st_yr, conv_s, conv_r, conv_m, conv_p, conv_y,
    loc, out_sem, a2a_rs, nr_rs, fw_rs, ya_rs, dp_rs, dy_rs, rt_rs, one_rs, sy_rs, cp_rs, cy_rs,
):
    e = lax.axis_index("ep")
    t = lax.axis_index("tp")
    y = t // 2
    c = t % 2
    partner = (e, y * 2 + (1 - c))
    feats = xbuf.shape[3]
    rows = n * cap
    per = n // groups
    near = near_groups * per

    def flip(v, d):
        bit = 1
        while bit <= d:
            if d & bit:
                v = v + bit - 2 * bit * lax.rem(v // bit, 2)
            bit *= 2
        return v

    def ep_peer(d):
        return (flip(e, d), t)

    def y_peer(m):
        return (e, lax.rem(y + m, ny) * 2 + c)

    def block_of(m, core):
        return lax.rem(y + ny - m, ny) * 2 + core

    def cols_of(block):
        return pl.ds(pl.multiple_of(block * feats, feats), feats)

    def remote(src, dst, rs, device):
        return pltpu.make_async_remote_copy(
            src_ref=src, dst_ref=dst, send_sem=out_sem.at[0], recv_sem=rs, device_id=device, device_id_type=MESH
        )

    pairs = dict(
        routes=(routes_h, routes), tok_b=(tokens_b_h, tok_b), gain_b=(gain_b_h, gain_b),
        tok_a=(tokens_a_h, tok_a), gain_a=(gain_a_h, gain_a), val=(value_h, val_w), gat=(gate_h, gat_w),
        taps=(taps_h, taps), eg=(eg_h.at[0], eg), eu=(eu_h.at[0], eu), ed=(ed_h.at[0], ed),
        chan=(chan_gain_h, chan_gain), out=(out_h, out_w), logits=(logits_h, logits),
    )
    local = {
        name: pltpu.make_async_copy(src, dst, loc.at[i]) for i, (name, (src, dst)) in enumerate(pairs.items())
    }
    for name in ("routes", "tok_b", "gain_b"):
        local[name].start()

    barrier = pltpu.get_barrier_semaphore()
    for d in range(n - 1, 0, -1):
        pl.semaphore_signal(barrier, inc=1, device_id=ep_peer(d), device_id_type=MESH)
    pl.semaphore_signal(barrier, inc=1, device_id=partner, device_id_type=MESH)
    for m in range(1, ny):
        pl.semaphore_signal(barrier, inc=1, device_id=y_peer(m), device_id_type=MESH)
    for name in list(pairs)[3:]:
        local[name].start()

    count = tok_b.shape[0]
    row = lax.broadcasted_iota(jnp.int32, (count, count), 0)
    col = lax.broadcasted_iota(jnp.int32, (count, count), 1)

    def upright(line):
        return jnp.sum(jnp.where(row == col, line, 0.0), axis=1, keepdims=True)

    local["routes"].wait()
    rel = jnp.bitwise_xor(routes[...], e).astype(F32)
    rel0, rel1 = upright(rel[0:1]), upright(rel[1:2])
    expert = lax.broadcasted_iota(jnp.int32, (count, n), 1).astype(F32)
    is0, is1 = expert == rel0, expert == rel1
    named = (jnp.where(is0, 1.0, 0.0) + jnp.where(is1, 1.0, 0.0)).astype(BF16)
    before = mm(jnp.where(row > col, 1.0, 0.0).astype(BF16), named)
    slot0 = rel0 * cap + jnp.sum(jnp.where(is0, before, 0.0), axis=1, keepdims=True)
    slot1 = rel1 * cap + jnp.sum(jnp.where(is1, before, 0.0), axis=1, keepdims=True)
    across0 = jnp.sum(jnp.where(row == col, slot0, 0.0), axis=0, keepdims=True)
    across1 = jnp.sum(jnp.where(row == col, slot1, 0.0), axis=0, keepdims=True)

    def picker(lo, hi):
        ids = lax.broadcasted_iota(jnp.int32, ((hi - lo) * cap, count), 0).astype(F32) + lo * cap
        return jnp.where((ids == across0) | (ids == across1), 1.0, 0.0).astype(BF16)

    local["tok_b"].wait()
    local["gain_b"].wait()
    whole = tok_b[...].astype(F32)
    scale_b = lax.rsqrt(jnp.mean(whole * whole, axis=1, keepdims=True) + 1e-06)

    def normed_b(block):
        at = cols_of(block)
        return (tok_b[:, at].astype(F32) * scale_b * gain_b[:, at]).astype(BF16)

    k0, k1, k2, k3 = chunks
    own = normed_b(t)

    def pick(lo, hi):
        send[lo:hi] = mm(picker(lo, hi), own).reshape(hi - lo, cap, feats).astype(BF16)

    pick(0, k0[1] * per)
    pick(k2[0] * per, k2[1] * per)
    pl.semaphore_wait(barrier, n + ny - 1)
    a2a, nears, crossings, forwards = {}, {}, {}, {}

    def dispatch(k):
        ds = list(range(max(1, k[0] * per), k[1] * per))
        for d in ds[::-1] if k is k3 else ds:
            a2a[d] = remote(send.at[d], xbuf.at[t, d], a2a_rs.at[d], ep_peer(d))
            a2a[d].start()

    dispatch(k0)
    dispatch(k2)
    pick(k0[1] * per, k2[0] * per)
    dispatch(k1)
    xbuf[t, 0] = send[0]

    pick_near, pick_own = picker(0, near), picker(0, 1)
    for m in range(1, ny):
        block = block_of(m, c)
        picked = mm(pick_near, normed_b(block)).reshape(near, cap, feats).astype(BF16)
        nsend[m] = picked
        xbuf[block, 0] = picked[0]

    def second(k):
        for m in range(1, ny):
            for d in range(max(1, k[0] * per), k[1] * per):
                to = xbuf.at[block_of(m, c), d]
                copy = remote(nsend.at[m, d], to, nr_rs.at[m - 1, d], ep_peer(d))
                copy.start()
                nears[m, d] = copy

    second(k0)
    for m in range(ny):
        block = block_of(m, 1 - c)
        xbuf[block, 0] = mm(pick_own, normed_b(block)).astype(BF16)

    def span(g):
        return max(1, g * per), (g + 1) * per

    def forward(m, g):
        lo, hi = span(g)
        if lo < hi:
            part = xbuf.at[block_of(m, c), pl.ds(lo, hi - lo)]
            copy = remote(part, part, fw_rs.at[m, g], partner)
            copy.start()
            forwards[m, g] = copy

    def arrive(g):
        lo, hi = span(g)
        for d in range(lo, hi):
            a2a[d].wait_recv()
        if g >= near_groups:
            part = xbuf.at[t, pl.ds(lo, hi - lo)]
            for m in range(1, ny):
                copy = remote(part, part, ya_rs.at[m - 1, g - near_groups], y_peer(m))
                copy.start()
                crossings[m, g] = copy
        forward(0, g)

    def hand_on(g):
        for m in range(1, ny):
            if g >= near_groups:
                crossings[m, g].wait_recv()
            else:
                for d in range(*span(g)):
                    nears[m, d].wait_recv()
            forward(m, g)

    def rows_of(k, block):
        lo, hi = k[0] * per, k[1] * per
        return xbuf[block, pl.ds(lo, hi - lo)].astype(F32).reshape((hi - lo) * cap, feats).astype(BF16)

    def accumulate(k, x, at, first):
        to = pl.ds(k[0] * per * cap, (k[1] - k[0]) * per * cap)
        if first:
            gacc[to, :] = mt(x, eg[:, at])
            uacc[to, :] = mt(x, eu[:, at])
        else:
            gacc[to, :] += mt(x, eg[:, at])
            uacc[to, :] += mt(x, eu[:, at])

    def project(k, block, first=False):
        accumulate(k, rows_of(k, block), cols_of(block), first)

    def forwarded(k, m):
        for g in range(*k):
            if (m, g) in forwards:
                forwards[m, g].wait_recv()

    def project_other(k):
        forwarded(k, 0)
        project(k, block_of(0, 1 - c))

    def project_pair(k, m, first=False):
        forwarded(k, m)
        base = lax.rem(y + ny - m, ny) * 2
        x = jnp.concatenate([rows_of(k, base), rows_of(k, base + 1)], axis=1)
        accumulate(k, x, pl.ds(pl.multiple_of(base * feats, 2 * feats), 2 * feats), first)

    def project_far(k):
        for m in range(1, ny):
            project_pair(k, m)

    def project_own(k):
        for m in range(1, ny):
            project(k, block_of(m, c))

    def project_last(k):
        for m in range(1, ny):
            forwarded(k, m)
            project(k, block_of(m, 1 - c))

    def out_cols(m, core):
        return cols_of(lax.rem(y + m, ny) * 2 + core)

    down_x, down_y, returns = {}, {}, {}
    order = list(range(1, ny)) + [0]

    def down(k):
        i = chunks.index(k)
        lo, hi = k[0] * per, k[1] * per
        to = pl.ds(lo * cap, (hi - lo) * cap)
        at = pl.ds(lo, hi - lo)
        hid = (jax.nn.silu(gacc[to, :]) * uacc[to, :]).astype(BF16)

        def product(m, core):
            return mm(hid, ed[:, out_cols(m, core)]).reshape(hi - lo, cap, feats)

        def exchange(m):
            copy = remote(down_s.at[m, at], down_r.at[m, at], dp_rs.at[m, i], partner)
            copy.start()
            down_x[m, i] = copy

        for m in order[:-1]:
            down_s[m, at] = product(m, 1 - c).astype(BF16)
            exchange(m)
        for m in order[:-1]:
            down_m[m, at] = product(m, c)
        down_s[0, at] = product(0, 1 - c).astype(BF16)
        down_m[0, at] = product(0, c)
        exchange(0)

    def cross_wait(k):
        for m in order[:-1]:
            down_x[m, chunks.index(k)].wait_recv()

    def cross_one(g):
        at = pl.ds(g * per, per)
        for m in order[:-1]:
            pair[m, at] = (down_m[m, at] + down_r[m, at].astype(F32)).astype(BF16)
            copy = remote(pair.at[m, at], yrecv.at[m, at], dy_rs.at[m - 1, g], y_peer(m))
            copy.start()
            down_y[m, g] = copy

    def cross(k):
        cross_wait(k)
        for g in reversed(range(*k)):
            cross_one(g)

    settled = []

    def give_back(*gs):
        for g in gs:
            i = [k[0] <= g < k[1] for k in chunks].index(True)
            if i not in settled:
                down_x[0, i].wait_recv()
                settled.append(i)
            at = pl.ds(g * per, per)
            summed = down_m[0, at] + down_r[0, at].astype(F32)
            for m in range(1, ny):
                down_y[m, g].wait_recv()
                summed = summed + yrecv[m, at].astype(F32)
            ret_s[at] = summed.astype(BF16)
            for d in range(g * per, (g + 1) * per):
                if d == 0:
                    ret_r[0] = summed[0].astype(BF16)
                else:
                    copy = remote(ret_s.at[d], ret_r.at[d], rt_rs.at[d], ep_peer(d))
                    copy.start()
                    returns[d] = copy

    local["tok_a"].wait()
    local["gain_a"].wait()
    whole = tok_a[...].astype(F32)
    scale = lax.rsqrt(jnp.mean(whole * whole, axis=1, keepdims=True) + 1e-06)
    normed = (whole * scale * gain_a[...]).astype(BF16)
    local["val"].wait()
    value = mm(normed, val_w[...])
    local["gat"].wait()
    glu = (value * jax.nn.sigmoid(mm(normed, gat_w[...]))).astype(BF16)
    length = glu.shape[0]
    tail[...] = glu[length - HALO:]
    rim = remote(tail, halo, one_rs.at[0], (lax.rem(e + 1, n), t))
    rim.start()
    dispatch(k3)
    second(k1)
    pad[HALO:] = glu.astype(F32)

    local["taps"].wait()
    width = taps.shape[0]
    chunk = min(128, pad.shape[1])

    def convolve(first, last):
        total = jnp.zeros((last - first, 1), F32)
        square = jnp.zeros((last - first, 1), F32)
        for lane in range(0, pad.shape[1], chunk):
            acc = jnp.zeros((last - first, chunk), F32)
            for tap in range(width):
                at = HALO - width + 1 + tap
                acc = acc + taps[tap:tap + 1, lane:lane + chunk] * pad[at + first:at + last, lane:lane + chunk]
            total = total + jnp.sum(acc, axis=1, keepdims=True)
            square = square + jnp.sum(acc * acc, axis=1, keepdims=True)
            mix[first:last, lane:lane + chunk] = acc
        return total, square

    rest_total, rest_square = convolve(HALO, length)

    local["eg"].wait()
    local["eu"].wait()
    if per > 1:
        arrive(0)
        hand_on(0)
    arrive(1)
    project(k0, t, True)
    hand_on(1)
    project_own(k0)
    arrive(6)
    project_other(k0)
    project_last(k0)
    arrive(7)
    local["ed"].wait()
    down(k0)
    project(k2, t, True)
    arrive(2)
    arrive(3)
    project(k1, t, True)
    project_other(k2)
    cross_wait(k0)
    cross_one(1)

    rim.wait_recv()
    pad[:HALO] = jnp.where(e > 0, halo[...].astype(F32), 0.0)
    rim_total, rim_square = convolve(0, HALO)
    total = jnp.concatenate([rim_total, rest_total], axis=0)
    square = jnp.concatenate([rim_square, rest_square], axis=0)
    lanes = lax.broadcasted_iota(jnp.int32, (length, 128), 1)
    stats = jnp.where(lanes < 4, total, square).T
    st_s[...] = stats[0:8]
    stat = remote(st_s, st_r, one_rs.at[1], partner)
    stat.start()

    hand_on(6)
    hand_on(7)
    project_own(k2)
    stat.wait_recv()
    st_ys[...] = st_s[...] + st_r[...]
    stat_y = []
    for m in range(1, ny):
        copy = remote(st_ys, st_yr.at[m], sy_rs.at[m - 1], y_peer(m))
        copy.start()
        stat_y.append(copy)
    arrive(5)
    project_last(k2)
    arrive(4)
    hand_on(2)
    hand_on(3)
    down(k2)
    project_other(k1)
    cross(k2)
    give_back(1)
    project_far(k1)
    down(k1)
    hand_on(5)
    project_pair(k3, 0, True)
    cross(k1)
    hand_on(4)
    project_own(k3)
    give_back(7)
    project_last(k3)
    down(k3)
    give_back(6)

    sums = st_ys[...]
    for m in range(1, ny):
        stat_y[m - 1].wait_recv()
        sums = sums + st_yr[m]
    local["chan"].wait()
    local["out"].wait()
    back = jnp.concatenate([sums] * (length // 8), axis=0).T
    average = back[:, 0:1] / channels
    spread = back[:, 4:5] / channels - average * average
    act = jax.nn.silu((mix[...] - average) * lax.rsqrt(spread + 1e-05) * chan_gain[...]).astype(BF16)

    cross(k3)
    cross_one(0)

    conv_x = []
    for m in range(ny):
        conv_s[m] = mm(act, out_w[:, out_cols(m, 1 - c)]).astype(BF16)
        copy = remote(conv_s.at[m], conv_r.at[m], cp_rs.at[m], partner)
        copy.start()
        conv_x.append(copy)
        conv_m[m] = mm(act, out_w[:, out_cols(m, c)])

    give_back(3)
    give_back(2)

    conv_cross = []
    for m in range(ny):
        conv_x[m].wait_recv()
        summed = conv_m[m] + conv_r[m].astype(F32)
        if m == 0:
            conv_m[0] = summed
        else:
            conv_p[m] = summed.astype(BF16)
            copy = remote(conv_p.at[m], conv_y.at[m], cy_rs.at[m - 1], y_peer(m))
            copy.start()
            conv_cross.append(copy)

    local["logits"].wait()
    logit = logits[...]
    top = jnp.max(logit, axis=0, keepdims=True)
    exps = jnp.exp(logit - top)
    weight = exps / jnp.sum(exps, axis=0, keepdims=True)
    weight0, weight1 = upright(weight[0:1]), upright(weight[1:2])

    def combined(k):
        lo, hi = k[0] * per, k[1] * per
        slots = lax.broadcasted_iota(jnp.int32, (count, (hi - lo) * cap), 1).astype(F32) + lo * cap
        combine = jnp.where(slots == slot0, weight0, 0.0) + jnp.where(slots == slot1, weight1, 0.0)
        high = combine.astype(BF16)
        low = (combine - high.astype(F32)).astype(BF16)
        for d in range(max(1, lo), hi):
            returns[d].wait_recv()
        came = ret_r[lo:hi].astype(F32).reshape((hi - lo) * cap, feats).astype(BF16)
        return mm(high, came) + mm(low, came)

    give_back(5)
    give_back(4)
    give_back(0)
    moved = combined(k0)
    moved = moved + combined(k1)
    moved = moved + combined(k2)

    result = conv_m[0]
    for m in range(1, ny):
        conv_cross[m - 1].wait_recv()
        result = result + conv_y[m].astype(F32)
    conv_o[...] = result.astype(BF16)

    middle = (k3[0] + k3[1]) // 2
    moved = moved + combined((middle, k3[1]))
    moe_o[...] = (moved + combined((k3[0], middle))).astype(BF16)

    sent = list(a2a.values()) + list(nears.values()) + list(crossings.values()) + list(forwards.values())
    sent += [rim, stat] + stat_y + conv_x + conv_cross
    sent += list(down_x.values()) + list(down_y.values()) + list(returns.values())
    for copy in sent:
        copy.wait_send()


def solution(mesh):
    n = mesh.shape["ep"]
    n_tp = mesh.shape["tp"]
    ny = n_tp // 2
    groups = 8
    if n % groups or n & (n - 1):
        raise ValueError("ep size")
    near_groups = 4
    chunks = [(0, 2), (2, 4), (6, 8), (4, 6)]

    def body(tokens_a, gain_a, value_w, gate_w, kernel, chan_gain, out_w,
             tokens_b, gain_b, routes, logits, eg, eu, ed):
        len_a, model = tokens_a.shape
        len_b = tokens_b.shape[0]
        chans = value_w.shape[1]
        feats = model // n_tp
        hidden = eg.shape[2]
        cap = 3 * len_b * routes.shape[1] // (2 * n)
        cap = -(-cap // 8) * 8
        rows = n * cap
        topk = routes.shape[1]
        near = near_groups * n // groups
        dma = pltpu.SemaphoreType.DMA
        vmem = pltpu.VMEM
        blocks = (n, cap, feats)
        scratch = [
            vmem((len_a, model), BF16), vmem((len_b, model), BF16),
            vmem((model, chans), BF16), vmem((model, chans), BF16), vmem((chans, model), BF16),
            vmem((hidden, model), BF16), vmem((hidden, model), BF16), vmem((hidden, model), BF16),
            vmem((1, model), F32), vmem((1, model), F32), vmem(kernel.shape, F32), vmem((1, chans), F32),
            vmem((topk, len_b), jnp.int32), vmem((topk, len_b), F32),
            vmem(blocks, BF16), vmem((ny, near, cap, feats), BF16), vmem((n_tp,) + blocks, BF16),
            vmem((rows, hidden), F32), vmem((rows, hidden), F32),
            vmem((ny,) + blocks, BF16), vmem((ny,) + blocks, BF16), vmem((ny,) + blocks, F32),
            vmem((ny,) + blocks, BF16), vmem((ny,) + blocks, BF16),
            vmem(blocks, BF16), vmem(blocks, BF16),
            vmem((HALO + len_a, chans), F32), vmem((len_a, chans), F32), vmem((HALO, chans), BF16), vmem((HALO, chans), BF16),
            vmem((8, len_a), F32), vmem((8, len_a), F32), vmem((8, len_a), F32), vmem((ny, 8, len_a), F32),
            vmem((ny, len_a, feats), BF16), vmem((ny, len_a, feats), BF16), vmem((ny, len_a, feats), F32),
            vmem((ny, len_a, feats), BF16), vmem((ny, len_a, feats), BF16),
            dma((14,)), dma((1,)), dma((n,)), dma((ny - 1, near)), dma((ny, groups)),
            dma((ny - 1, groups - near_groups)), dma((ny, 4)), dma((ny - 1, groups)), dma((n,)),
            dma((2,)), dma((ny - 1,)), dma((ny,)), dma((ny - 1,)),
        ]
        hbm = pl.BlockSpec(memory_space=pl.ANY)
        here = pl.BlockSpec(memory_space=vmem)
        conv, moe = pl.pallas_call(
            functools.partial(kernel_body, n, ny, cap, groups, near_groups, chunks, chans * n_tp),
            out_shape=(
                vmem((len_a, feats), BF16),
                vmem((len_b, feats), BF16),
            ),
            in_specs=[hbm] * 14,
            out_specs=(here, here),
            scratch_shapes=scratch,
            compiler_params=pltpu.CompilerParams(
                collective_id=0, has_side_effects=True, vmem_limit_bytes=62914560
            ),
        )(tokens_a, gain_a[None, :], value_w, gate_w, kernel, chan_gain[None, :], out_w,
          tokens_b, gain_b[None, :], routes.T, logits.T, eg.swapaxes(1, 2), eu.swapaxes(1, 2), ed)

        def finish(conv_i, moe_i, conv_f, moe_f):
            conv_f[...] = conv_i[...].T
            moe_f[...] = moe_i[...]

        conv, moe = pl.pallas_call(
            finish,
            out_shape=(
                jax.ShapeDtypeStruct((feats, len_a), BF16),
                jax.ShapeDtypeStruct((len_b, feats), BF16),
            ),
            in_specs=[here, here],
            out_specs=(here, here),
            compiler_params=pltpu.CompilerParams(vmem_limit_bytes=4 * 1024 * 1024),
        )(conv, moe)
        return conv, moe.T

    return jax.shard_map(
        body,
        mesh=mesh,
        in_specs=(
            P("ep", None), P(), P(None, "tp"), P(None, "tp"), P(None, "tp"), P("tp"), P("tp", None),
            P("ep", None), P(), P("ep", None), P("ep", None),
            P("ep", None, "tp"), P("ep", None, "tp"), P("ep", "tp", None),
        ),
        out_specs=(P("tp", "ep"), P("tp", "ep")),
        check_vma=False,
    )
```
